256 devices in a mesh: sp: 64 (over z, y, core), tp: 4 (over x).
Axes of the slice: x: 4, y: 4, z: 8, core: 2. Of those that a mesh axis runs over, the one named last changes fastest.
Arguments:
- residual: bfloat16 [16384, 2048], P(('sp', 'tp')), may hold values from -6 to 6
- queries: bfloat16 [16384, 2048], P('sp', 'tp'), may hold values from -40 to 40
- key_rows: bfloat16 [16384, 1024], P('sp', 'tp'), may hold values from -40 to 40
- value_rows: bfloat16 [16384, 1024], P('sp', 'tp'), may hold values from -6 to 6
- forget_sums: float32 [16384, 16], P('sp', 'tp'), as said below
- out_weight: bfloat16 [2048, 2048], P('tp'), may hold values from -0.25 to 0.25
- norm_gain: float32 [2048], replicated, may hold values from 0.1 to 1.9
- expert_ids: int32 [16384, 4], P(('sp', 'tp')), may hold values from 0 to 63, all different within a row; in each aligned block of 64 rows (0 to 63, 64 to 127, ...) at most 8 rows name the same one
- route_weights: float32 [16384, 4], P(('sp', 'tp')), may hold values from 0.1 to 1
- expert_gate: bfloat16 [64, 2048, 384], P('sp'), may hold values from -0.125 to 0.125
- expert_up: bfloat16 [64, 2048, 384], P('sp'), may hold values from -0.125 to 0.125
- expert_down: bfloat16 [64, 384, 2048], P('sp'), may hold values from -0.3125 to 0.3125
- shared_gate: bfloat16 [2048, 384], replicated, may hold values from -0.125 to 0.125
- shared_up: bfloat16 [2048, 384], replicated, may hold values from -0.125 to 0.125
- shared_down: bfloat16 [384, 2048], replicated, may hold values from -0.3125 to 0.3125
Outputs:
- layer_out: bfloat16 [16384, 2048], P(('sp', 'tp'))
The draws below stay inside these ranges and needn't reach their ends.
Inputs may be any that keep to these rules, and one draw needn't show every extreme that they name: `forget_sums`: each head's column never rises from one position to the next. `expert_ids`: each row names 4 different experts; among the rows of one device no expert is named more than 8 times.
All inputs are finite; a program needn't handle non-finite values.
Results may differ from the reference program's by a relative error of at most 0.014.
Values may be sent and summed in bfloat16 or wider, within the bound.
A program may use at most 128 MiB of HBM per device.

```python
import math
import jax
import jax.numpy as jnp
import numpy as np
from jax import lax

D = 2048
HEADS = 16
KV_HEADS = 8
HEAD_DIM = 128
FE = 384
FS = 384
TOPK = 4
TOK_DEV = 256
EXPERTS = 64
TOKENS = 16384
ROWS = 64
CAP = 8


def query_key_pair(key):
    base_seed = jax.random.fold_in(key, 11)
    seed_list = jax.random.split(base_seed, 2)
    query_rows = 1.3 * jax.random.normal(seed_list[0], (TOKENS, HEADS * HEAD_DIM), jnp.float32)
    key_block = 1.3 * jax.random.normal(seed_list[1], (TOKENS, KV_HEADS * HEAD_DIM), jnp.float32)
    return (jnp.clip(query_rows, -40.0, 40.0), jnp.clip(key_block, -40.0, 40.0))


def draw_queries(key, part):
    return query_key_pair(key)[0].astype(jnp.bfloat16)


def draw_key_rows(key, part):
    return query_key_pair(key)[1].astype(jnp.bfloat16)


def draw_forget_sums(key, part):
    base_seed = jax.random.fold_in(key, 23)
    seed_list = jax.random.split(base_seed, 7)
    ordering = jax.random.permutation(seed_list[0], HEADS)
    slowly = ordering < HEADS // 2
    slow_rate = jax.random.uniform(seed_list[1], (HEADS,), jnp.float32, 0.25, 1.0) / TOKENS
    fast_rate = jnp.exp(jax.random.uniform(seed_list[2], (HEADS,), jnp.float32, math.log(0.01), math.log(1.0 / 30.0)))
    rates = jnp.where(slowly, slow_rate, fast_rate)
    block_count = TOKENS // TOK_DEV
    factor = jnp.exp(jax.random.uniform(seed_list[3], (block_count, 1), jnp.float32, -0.7, 0.7))
    factor = jnp.repeat(factor, TOK_DEV, axis=0)
    rough = jax.random.uniform(seed_list[4], (TOKENS, HEADS), jnp.float32, 0.2, 1.8)
    log_steps = -rates[None, :] * factor * rough
    places = jax.random.randint(seed_list[5], (3,), 0, TOKENS)
    losses = jnp.log(jax.random.uniform(seed_list[6], (3, HEADS), jnp.float32, 0.5, 0.8))
    log_steps = log_steps.at[places].add(jnp.where(slowly[None, :], losses, 0.0))
    return jnp.cumsum(log_steps, axis=0)


def block_levels(rng, dims, pieces, smallest, high):
    factor_of, own = 1.0, jax.random.fold_in(rng, 6)
    for dim, parts in pieces:
        heights = jnp.exp(jax.random.uniform(jax.random.fold_in(own, dim), (parts,), jnp.float32, smallest / len(pieces), high / len(pieces)))
        factor_of = factor_of * jnp.repeat(heights, dims[dim] // parts).reshape([-1 if axis == dim else 1 for axis in range(len(dims))])
    return factor_of


def assign_block(own_key, own, number, rows, count, top, most, skew):
    sequence = jax.random.permutation(own_key, count)
    crowded, common = load_shares(count, rows * top, most, skew, True), load_shares(count, rows * top, most, skew, False)
    places = jnp.arange(count)

    def named(lengths, rotation):
        used = int((lengths > 0).sum())
        fixed = max(1, used // 4)
        moved = fixed + (places - fixed + rotation * (used - fixed)) % max(1, count - fixed)
        return jnp.zeros((count,), jnp.int32).at[sequence[jnp.where(places < fixed, places, moved)]].set(jnp.asarray(lengths, jnp.int32))

    lengths = jnp.where(number % 4 == 0, named(crowded, number // 4), named(common, number - number // 4 - 1))
    mixed = jax.random.permutation(jax.random.fold_in(own, 3), count)
    source_of, receiver = mixed[0:count // 2 * 2:2], mixed[1:count // 2 * 2:2]
    margin = jnp.minimum(lengths[source_of] - 1, most - lengths[receiver]) // 2
    margin = jnp.where((source_of == sequence[0]) | (receiver == sequence[0]) | (lengths[receiver] == 0), 0, jnp.maximum(margin, 0))
    moved = jax.random.randint(jax.random.fold_in(own, 4), (count // 2,), 0, 1 << 20) % (margin + 1)
    lengths = lengths.at[source_of].add(-moved).at[receiver].add(moved)
    labels = jnp.searchsorted(jnp.cumsum(lengths), jnp.arange(rows * top), side="right").astype(jnp.int32)
    grid = labels.reshape(top, rows).T
    grid = grid[jax.random.permutation(jax.random.fold_in(own, 1), rows)]
    rotation = jax.random.randint(jax.random.fold_in(own, 2), (rows, 1), 0, top)
    return jnp.take_along_axis(grid, (jnp.arange(top)[None, :] + rotation) % top, axis=1)


def load_shares(count, total, reach, lean, full):
    weights = [(1 << 20) // math.isqrt(grade ** lean) + 1 for grade in range(1, count + 1)]
    largest = reach if full else min(reach, max(-(-total // count), total * weights[0] // sum(weights)))
    least = 1 if total - largest >= count - 1 else 0
    given, surplus = [largest] + [least] * (count - 1), total - largest - least * (count - 1)
    while surplus > 0:
        free = [i for i in range(1, count) if given[i] < largest] or [i for i in range(1, count) if given[i] < reach]
        whole, budget = sum([weights[i] for i in free]), surplus
        for i in free:
            more = min(reach - given[i], max(1, budget * weights[i] // whole), surplus)
            given[i] = given[i] + more
            surplus = surplus - more
    return np.array(given)


def scatter_about(own_key, extent, scale, limit, cuts=(), held_as=jnp.bfloat16):
    values = scale * jax.random.normal(own_key, extent, jnp.float32)
    if cuts:
        values = values * block_levels(own_key, extent, cuts, -0.22, 0.18)
    return jnp.clip(values, -limit, limit).astype(held_as)


def setup_inputs(seed: int = 0) -> dict:
    splits = jax.random.split(jax.random.key(seed), 16)
    residual = scatter_about(splits[0], (TOKENS, D), 1.0, 6.0, ((0, 256),))
    queries = draw_queries(jax.random.fold_in(splits[15], 71), 0)
    key_rows = draw_key_rows(jax.random.fold_in(splits[15], 71), 0)
    value_rows = scatter_about(splits[3], (TOKENS, KV_HEADS * HEAD_DIM), 1.0, 6.0, ((0, 64), (1, 4)))
    forget_sums = draw_forget_sums(jax.random.fold_in(splits[15], 71), 0)
    out_weight = scatter_about(splits[5], (HEADS * HEAD_DIM, D), (HEADS * HEAD_DIM // 4) ** -0.5, 0.25, ((0, 4),))
    norm_gain = jnp.clip(1.0 + 0.18 * jax.random.normal(splits[6], (D,), jnp.float32), 0.1, 1.9)
    expert_ids_keys = jax.random.split(jax.random.fold_in(splits[7], 1), TOKENS // ROWS)
    expert_ids_turns = jax.random.permutation(jax.random.fold_in(splits[7], 3), TOKENS // ROWS)
    expert_ids = jax.vmap(lambda own, number: assign_block(jax.random.fold_in(splits[7], 2), own, number, ROWS, EXPERTS, TOPK, CAP, 2))(expert_ids_keys, expert_ids_turns).reshape((TOKENS, TOPK))
    route_weights = jnp.clip(jnp.exp(math.log(1.0) - 2.3025851 * jax.random.uniform(splits[8], (TOKENS, TOPK), jnp.float32) ** block_levels(splits[8], (TOKENS, TOPK), ((0, 256),), -0.2, 0.2)), 0.1, 1.0)
    expert_gate = scatter_about(splits[9], (EXPERTS, D, FE), D ** -0.5, 0.125, ((0, 64),))
    expert_up = scatter_about(splits[10], (EXPERTS, D, FE), D ** -0.5, 0.125, ((0, 64),))
    expert_down = scatter_about(splits[11], (EXPERTS, FE, D), FE ** -0.5, 0.3125, ((0, 64),))
    shared_gate = scatter_about(splits[12], (D, FS), D ** -0.5, 0.125)
    shared_up = scatter_about(splits[13], (D, FS), D ** -0.5, 0.125)
    shared_down = scatter_about(splits[14], (FS, D), FS ** -0.5, 0.3125)
    return {"residual": residual, "queries": queries, "key_rows": key_rows, "value_rows": value_rows, "forget_sums": forget_sums, "out_weight": out_weight, "norm_gain": norm_gain, "expert_ids": expert_ids, "route_weights": route_weights, "expert_gate": expert_gate, "expert_up": expert_up, "expert_down": expert_down, "shared_gate": shared_gate, "shared_up": shared_up, "shared_down": shared_down}


routed_scale = 2.5
norm_eps = 1e-06

def attend(queries, key_rows, value_rows, forget_sums):
    group_size = HEADS // KV_HEADS
    score_scale = HEAD_DIM ** (-0.5)
    key_heads = key_rows.astype(jnp.float32).reshape(TOKENS, KV_HEADS, HEAD_DIM)
    value_heads = value_rows.astype(jnp.float32).reshape(TOKENS, KV_HEADS, HEAD_DIM)
    key_sums = forget_sums.reshape(TOKENS, KV_HEADS, group_size).transpose(1, 2, 0)
    positions = jnp.arange(TOKENS, dtype=jnp.int32)
    block_rows = math.gcd(TOKENS, 256)

    def one_block(first_pos):
        query_block = lax.dynamic_slice_in_dim(queries, first_pos, block_rows, 0).astype(jnp.float32)
        query_block = query_block.reshape(block_rows, KV_HEADS, group_size, HEAD_DIM)
        query_sums = lax.dynamic_slice_in_dim(forget_sums, first_pos, block_rows, 0)
        query_sums = query_sums.reshape(block_rows, KV_HEADS, group_size).transpose(1, 2, 0)
        scores = jnp.einsum('qhgd,khd->hgqk', query_block, key_heads) * score_scale
        scores = scores + (query_sums[:, :, :, None] - key_sums[:, :, None, :])
        query_pos = first_pos + jnp.arange(block_rows, dtype=jnp.int32)
        allowed = query_pos[:, None] >= positions[None, :]
        scores = jnp.where(allowed, scores, -jnp.inf)
        row_max = lax.optimization_barrier(jnp.max(scores, axis=3, keepdims=True))
        weights = jnp.exp(scores - row_max)
        weight_sum = lax.optimization_barrier(jnp.sum(weights, axis=3))
        rounded = lax.optimization_barrier(weights.astype(jnp.bfloat16)).astype(jnp.float32)
        mixed = jnp.einsum('hgqk,khd->qhgd', rounded, value_heads)
        mixed = mixed / weight_sum.transpose(2, 0, 1)[:, :, :, None]
        return mixed.reshape(block_rows, HEADS * HEAD_DIM).astype(jnp.bfloat16)
    starts = jnp.arange(TOKENS // block_rows, dtype=jnp.int32) * block_rows
    return lax.map(one_block, starts).reshape(TOKENS, HEADS * HEAD_DIM)

def experts_all(normed, expert_ids, route_weights, expert_gate, expert_up, expert_down):
    slot_count = TOKENS // ROWS * CAP
    flat_ids = expert_ids.reshape(-1)
    assigned = flat_ids.shape[0]
    gates = route_weights / lax.optimization_barrier(jnp.sum(route_weights, axis=1, keepdims=True)) * routed_scale
    flat_gates = jnp.concatenate([gates.reshape(-1), jnp.zeros((1,), jnp.float32)])
    padded = jnp.concatenate([normed, jnp.zeros((1, D), jnp.bfloat16)])

    def one_expert(carried, expert):
        chosen = flat_ids == expert
        place = jnp.where(chosen, jnp.cumsum(chosen.astype(jnp.int32)) - 1, slot_count)
        source = jnp.full((slot_count + 1,), assigned, jnp.int32)
        source = source.at[place].set(jnp.arange(assigned, dtype=jnp.int32))[:slot_count]
        token_rows = padded[source // TOPK]
        gate_part = jnp.dot(token_rows, expert_gate[expert], preferred_element_type=jnp.float32)
        up_part = jnp.dot(token_rows, expert_up[expert], preferred_element_type=jnp.float32)
        hidden = (jax.nn.silu(gate_part) * up_part).astype(jnp.bfloat16)
        output = jnp.dot(hidden, expert_down[expert], preferred_element_type=jnp.float32).astype(jnp.bfloat16)
        carried = carried.at[source // TOPK].add(flat_gates[source][:, None] * output.astype(jnp.float32))
        return (carried, None)
    routed, _ = lax.scan(one_expert, jnp.zeros((TOKENS + 1, D), jnp.float32), jnp.arange(EXPERTS, dtype=jnp.int32))
    return routed[:TOKENS]

def reference(residual, queries, key_rows, value_rows, forget_sums, out_weight, norm_gain, expert_ids, route_weights, expert_gate, expert_up, expert_down, shared_gate, shared_up, shared_down):
    attended = attend(queries, key_rows, value_rows, forget_sums)
    branch = jnp.dot(attended, out_weight, preferred_element_type=jnp.float32)
    stream = (residual.astype(jnp.float32) + branch).astype(jnp.bfloat16)
    wide = lax.optimization_barrier(stream).astype(jnp.float32)
    normed = (wide * lax.rsqrt(lax.optimization_barrier(jnp.mean(wide * wide, axis=1, keepdims=True)) + norm_eps) * norm_gain).astype(jnp.bfloat16)
    routed = experts_all(normed, expert_ids, route_weights, expert_gate, expert_up, expert_down)
    shared_hidden = (jax.nn.silu(jnp.dot(normed, shared_gate, preferred_element_type=jnp.float32)) * jnp.dot(normed, shared_up, preferred_element_type=jnp.float32)).astype(jnp.bfloat16)
    shared_out = jnp.dot(shared_hidden, shared_down, preferred_element_type=jnp.float32)
    return (wide + shared_out + routed).astype(jnp.bfloat16)
```

```python
import functools
import math

import jax
import jax.numpy as jnp
from jax import lax
from jax.experimental import pallas as pl
from jax.experimental.pallas import tpu as pltpu
from jax.sharding import PartitionSpec as P

HEADS = 16
KV_HEADS = 8
HEAD_DIM = 128
TOPK = 4
MESH = pl.DeviceIdType.MESH
LOG2E = 1.4426950408889634
NEG = -1e30

routed_scale = 2.5
norm_eps = 1e-06

NZ, NY, NX = 8, 4, 4
UP_STEPS, DOWN_STEPS = 4, 3


def attention_kernel(
    q_in,
    k_in,
    v_in,
    f_in,
    w_in,
    res_ref,
    gain_ref,
    stream_ref,
    normed_ref,
    qbuf,
    fqbuf,
    kbuf,
    vbuf,
    fbuf,
    bias,
    acc,
    stats,
    obuf,
    lbuf,
    rbuf,
    lrecv,
    wcols,
    att,
    wbuf,
    q_send,
    q_recv,
    kv_send,
    kv_recv,
    o_send,
    o_recv,
    l_send,
    l_recv,
    w_send,
    w_recv,
    p_send,
    p_recv,
    local_sem,
):
    sp = lax.axis_index("sp")
    x = lax.axis_index("tp")
    z = sp // 8
    me8 = sp % 8
    y = me8 // 2
    c = me8 % 2
    zbase = z * 8

    def at_z(step, core):
        return ((z + step + NZ) % NZ) * 8 + y * 2 + core

    partner = zbase + y * 2 + (1 - c)
    xr = (x + 1) % NX
    xl = (x + NX - 1) % NX

    barrier = pltpu.get_barrier_semaphore()

    def greet_plane(i, _):
        n = i + 1
        r8, rx = n // NX, n % NX
        pl.semaphore_signal(
            barrier,
            inc=1,
            device_id=(zbase + (me8 + r8) % 8, (x + rx) % NX),
            device_id_type=MESH,
        )
        return 0

    lax.fori_loop(0, 31, greet_plane, 0)
    for step in (1, -1):
        for core in (0, 1):
            pl.semaphore_signal(
                barrier, inc=1, device_id=(at_z(step, core), x), device_id_type=MESH
            )
    pl.semaphore_wait(barrier, 35)

    def remote(src, dst, send, recv, sp_id, tp_id):
        return pltpu.make_async_remote_copy(
            src_ref=src,
            dst_ref=dst,
            send_sem=send,
            recv_sem=recv,
            device_id=(sp_id, tp_id),
            device_id_type=MESH,
        )

    kv_arrays = ((k_in, kbuf), (v_in, vbuf), (f_in, fbuf))
    first_sends = []
    for a in (2, 0, 1):
        src, dst = kv_arrays[a]
        pltpu.make_async_copy(src.at[c], dst.at[0, c], local_sem.at[a]).start()
        first_sends.append(
            remote(
                src.at[1 - c],
                dst.at[0, c],
                kv_send.at[a, 0, 0],
                kv_recv.at[a, 0, 0],
                partner,
                x,
            )
        )
        for step, slot in ((1, 1), (-1, 1 + UP_STEPS)):
            for h in (0, 1):
                first_sends.append(
                    remote(
                        src.at[h],
                        dst.at[slot, c],
                        kv_send.at[a, slot, h],
                        kv_recv.at[a, slot, c],
                        at_z(step, h),
                        x,
                    )
                )
    for copy in first_sends:
        copy.start()

    pltpu.make_async_copy(q_in.at[c], qbuf.at[me8], local_sem.at[3]).start()
    pltpu.make_async_copy(f_in.at[c], fqbuf.at[me8], local_sem.at[4]).start()
    pltpu.make_async_copy(w_in, wbuf.at[x], local_sem.at[5]).start()

    def q_copies(r):
        to = (me8 + r) % 8
        return (
            remote(f_in.at[to % 2], fqbuf.at[me8], q_send.at[1, r], q_recv.at[1, r], zbase + to, x),
            remote(q_in.at[to % 2], qbuf.at[me8], q_send.at[0, r], q_recv.at[0, r], zbase + to, x),
        )

    def start_q(i, _):
        for copy in q_copies(i + 1):
            copy.start()
        return 0

    lax.fori_loop(0, 7, start_q, 0)

    quarter = w_in.shape[0] // 4
    rows_a = pl.ds(c * 2 * quarter, quarter)
    rows_b = pl.ds(c * 2 * quarter + quarter, quarter)
    rows_half = pl.ds(c * 2 * quarter, 2 * quarter)
    across = (x + 2) % NX
    w_first = [
        remote(w_in.at[rows_a], wbuf.at[x, rows_a], w_send.at[0], w_recv.at[0], sp, xr),
        remote(w_in.at[rows_b], wbuf.at[x, rows_b], w_send.at[2], w_recv.at[2], sp, xl),
        remote(w_in.at[rows_b], wbuf.at[x, rows_b], w_send.at[1], w_recv.at[1], sp, xr),
        remote(w_in.at[rows_a], wbuf.at[x, rows_a], w_send.at[3], w_recv.at[3], sp, xl),
    ]
    for copy in w_first:
        copy.start()
    w_forward = [
        remote(wbuf.at[xl, rows_a], wbuf.at[xl, rows_a], w_send.at[4], w_recv.at[4], sp, xr),
        remote(wbuf.at[xr, rows_b], wbuf.at[xr, rows_b], w_send.at[5], w_recv.at[5], sp, xl),
    ]
    w_partner = [
        remote(wbuf.at[o, rows_half], wbuf.at[o, rows_half], p_send.at[i], p_recv.at[i], partner, x)
        for i, o in enumerate((xl, xr, across))
    ]

    acc[...] = jnp.zeros_like(acc)
    row = lax.broadcasted_iota(jnp.int32, stats.shape, 1)
    stats[...] = jnp.where(row < 2, NEG, 0.0)

    scale = HEAD_DIM ** (-0.5) * LOG2E

    def make_bias(slot):
        f0 = fbuf[slot, 0]
        base = f0[:, 0:1]
        for cc in (0, 1):
            f = f0 if cc == 0 else fbuf[slot, 1]
            b = (base - f) * LOG2E
            bias[cc] = jnp.concatenate([b] * 16, axis=0).T

    def task(slot, qb, masked):
        if masked:
            rows = lax.broadcasted_iota(jnp.int32, (256, 256), 0)
            cols = lax.broadcasted_iota(jnp.int32, (256, 256), 1)
            gap = (qb - 2 * y) * 256
        for h in (0, 1):
            q_h = qbuf[qb, h * 128 : (h + 1) * 128, :]
            delta = (fqbuf[qb, h : h + 1, 0:1] - fbuf[slot, 0, h : h + 1, 0:1]) * LOG2E
            scores = []
            for cc in (0, 1):
                s = jnp.dot(kbuf[slot, cc], q_h, preferred_element_type=jnp.float32)
                s = s * scale + bias[cc, :, h : h + 1]
                if masked:
                    s = jnp.where(rows + cc * 256 <= cols + gap, s, -jnp.inf)
                scores.append(s)
            top = jnp.max(jnp.maximum(scores[0], scores[1]), axis=0, keepdims=True)
            old = stats[qb, h : h + 1, :]
            new = jnp.maximum(old, top + delta)
            shift = new - delta
            factor = jnp.exp2(old - new)
            p = [jnp.exp2(s - shift) for s in scores]
            total = jnp.sum(p[0] + p[1], axis=0, keepdims=True)
            stats[qb, h : h + 1, :] = new
            stats[qb, 2 + h : 3 + h, :] = stats[qb, 2 + h : 3 + h, :] * factor + total
            mixed = jnp.dot(
                vbuf[slot, 0], p[0].astype(jnp.bfloat16), preferred_element_type=jnp.float32
            ) + jnp.dot(
                vbuf[slot, 1], p[1].astype(jnp.bfloat16), preferred_element_type=jnp.float32
            )
            acc[qb, h] = acc[qb, h] * factor + mixed

    def wait_first(a, slot):
        for h in (0, 1):
            remote(
                kv_arrays[a][0].at[h],
                kv_arrays[a][1].at[slot, h],
                kv_send.at[a, slot, h],
                kv_recv.at[a, slot, h],
                partner,
                x,
            ).wait_recv()

    def forward(a, slot, step):
        buf = kv_arrays[a][1]
        return remote(
            buf.at[slot],
            buf.at[slot + 1],
            kv_send.at[a, slot + 1, 0],
            kv_recv.at[a, slot + 1, 0],
            at_z(step, c),
            x,
        )

    forwards = []

    def arrive(slot, step, first, send_on):
        for a in (2, 0, 1):
            if first:
                wait_first(a, slot)
            else:
                forward(a, slot - 1, step).wait_recv()
            if send_on:
                copy = forward(a, slot, step)
                copy.start()
                forwards.append(copy)

    def absorb(slot, origin_ok):
        @pl.when(origin_ok)
        def _():
            make_bias(slot)

            def body(qb, _):
                task(slot, qb, False)
                return 0

            lax.fori_loop(0, 8, body, 0)

    for a in range(3):
        pltpu.make_async_copy(
            kv_arrays[a][0].at[c], kv_arrays[a][1].at[0, c], local_sem.at[a]
        ).wait()
        remote(
            kv_arrays[a][0].at[1 - c],
            kv_arrays[a][1].at[0, c],
            kv_send.at[a, 0, 0],
            kv_recv.at[a, 0, 0],
            partner,
            x,
        ).wait_recv()
    pltpu.make_async_copy(q_in.at[c], qbuf.at[me8], local_sem.at[3]).wait()
    pltpu.make_async_copy(f_in.at[c], fqbuf.at[me8], local_sem.at[4]).wait()
    arrive(1, 1, True, True)
    arrive(1 + UP_STEPS, -1, True, True)
    make_bias(0)

    def own(r, _):
        @pl.when(r > 0)
        def _():
            for copy in q_copies(jnp.maximum(r, 1)):
                copy.wait_recv()

        qb = (me8 + 8 - r) % 8

        @pl.when(qb // 2 >= y)
        def _():
            task(0, qb, True)

        return 0

    lax.fori_loop(0, 8, own, 0)
    w_first[0].wait_recv()
    w_forward[0].start()
    w_first[2 - 1].wait_recv()
    w_forward[1].start()
    absorb(1, z >= 1)
    absorb(5, z + 1 >= NZ)
    arrive(2, 1, False, True)
    arrive(6, -1, False, True)
    absorb(2, z >= 2)
    absorb(6, z + 2 >= NZ)
    arrive(3, 1, False, True)
    arrive(7, -1, False, False)
    w_first[2].wait_recv()
    w_partner[0].start()
    w_first[3].wait_recv()
    w_partner[1].start()
    absorb(3, z >= 3)
    absorb(7, z + 3 >= NZ)
    arrive(4, 1, False, False)
    absorb(4, z >= 4)
    w_forward[0].wait_recv()
    w_forward[1].wait_recv()
    w_partner[2].start()

    def o_copy(r8, rx):
        to = (me8 + r8) % 8
        tx = (x + rx) % NX
        return (
            remote(
                obuf.at[to, pl.ds(tx * 64, 64)],
                rbuf.at[y, :, pl.ds((x * 2 + c) * 256, 256)],
                o_send.at[r8, rx],
                o_recv.at[r8, rx],
                zbase + to,
                tx,
            ),
            remote(
                lbuf.at[to, tx // 2],
                lrecv.at[y, x * 2 + c],
                l_send.at[r8, rx],
                l_recv.at[r8, rx],
                zbase + to,
                tx,
            ),
        )

    def finish(r, _):
        r8 = 7 - r
        qb = (me8 + r8) % 8
        sums = []
        for h in (0, 1):
            total = stats[qb, 2 + h : 3 + h, :]
            some = total > 0.0
            inv = jnp.where(some, 1.0 / jnp.where(some, total, 1.0), 0.0)
            obuf[qb, :, h * 128 : (h + 1) * 128] = (acc[qb, h] * inv).T.astype(jnp.bfloat16)
            sums.append(
                jnp.where(
                    some, stats[qb, h : h + 1, :] + jnp.log2(jnp.where(some, total, 1.0)), NEG
                )
            )
        both = jnp.concatenate(sums + [jnp.zeros((6, 256), jnp.float32)], axis=0)
        lbuf[qb, 0] = both[:, :128]
        lbuf[qb, 1] = both[:, 128:]
        for rx in (2, 1, 3):
            for copy in o_copy(r8, rx):
                copy.start()

        @pl.when(r8 > 0)
        def _():
            for copy in o_copy(r8, 0):
                copy.start()

        return 0

    lax.fori_loop(0, 8, finish, 0)
    own_copies = (
        pltpu.make_async_copy(
            obuf.at[me8, pl.ds(x * 64, 64)],
            rbuf.at[y, :, pl.ds((x * 2 + c) * 256, 256)],
            local_sem.at[6],
        ),
        pltpu.make_async_copy(lbuf.at[me8, x // 2], lrecv.at[y, x * 2 + c], local_sem.at[7]),
    )
    for copy in own_copies:
        copy.start()
    for copy in own_copies:
        copy.wait()

    def wait_o(r, _):
        for copy in o_copy((r + 1) // NX, (r + 1) % NX):
            copy.wait_recv()
        return 0

    lax.fori_loop(0, 31, wait_o, 0)

    logs = [lrecv[i].reshape(64, 128) for i in range(NY)]
    top = jnp.maximum(jnp.maximum(logs[0], logs[1]), jnp.maximum(logs[2], logs[3]))
    parts = [jnp.exp2(v - top) for v in logs]
    inv = 1.0 / (parts[0] + parts[1] + parts[2] + parts[3])
    for i in range(NY):
        scaled = parts[i] * inv
        wcols[i] = jnp.concatenate([scaled, scaled], axis=0).T
    first_row = pl.multiple_of((x % 2) * 64, 64)
    shares = [wcols[i, pl.ds(first_row, 64), :] for i in range(NY)]
    for n in range(HEADS):
        lane = (n // 2) * 8 + n % 2
        cols = slice(n * 128, (n + 1) * 128)
        mixed = shares[0][:, lane : lane + 1] * rbuf[0, :, cols].astype(jnp.float32)
        for i in range(1, NY):
            mixed = mixed + shares[i][:, lane : lane + 1] * rbuf[i, :, cols].astype(jnp.float32)
        att[:, cols] = mixed.astype(jnp.bfloat16)

    pltpu.make_async_copy(w_in, wbuf.at[x], local_sem.at[5]).wait()
    for copy in w_partner:
        copy.wait_recv()

    width = w_in.shape[1]
    chunk = 256

    def project(i, total):
        cols = pl.ds(pl.multiple_of(i * chunk, chunk), chunk)
        part = jnp.dot(att[:, 0:512], wbuf[0, :, cols], preferred_element_type=jnp.float32)
        for b in range(1, NX):
            part = part + jnp.dot(
                att[:, b * 512 : (b + 1) * 512],
                wbuf[b, :, cols],
                preferred_element_type=jnp.float32,
            )
        stream = (res_ref[:, cols].astype(jnp.float32) + part).astype(jnp.bfloat16)
        stream_ref[:, cols] = stream
        wide = stream.astype(jnp.float32)
        return total + jnp.sum(wide * wide, axis=1, keepdims=True)

    total = lax.fori_loop(0, width // chunk, project, jnp.zeros((64, 1), jnp.float32))
    rate = lax.rsqrt(total * (1.0 / width) + norm_eps)
    normed_ref[...] = (stream_ref[...].astype(jnp.float32) * rate * gain_ref[...]).astype(
        jnp.bfloat16
    )

    for copy in first_sends + forwards + w_first + w_forward + w_partner:
        copy.wait_send()

    def wait_q(i, _):
        for copy in q_copies(i + 1):
            copy.wait_send()
        return 0

    lax.fori_loop(0, 7, wait_q, 0)

    def wait_sent(r, _):
        for copy in o_copy((r + 1) // NX, (r + 1) % NX):
            copy.wait_send()
        return 0

    lax.fori_loop(0, 31, wait_sent, 0)


def attention(residual, queries, key_rows, value_rows, forget_sums, out_weight, norm_gain):
    rows, width = residual.shape
    tokens = queries.shape[0]
    q_in = queries.T.reshape(2, 256, tokens)
    k_in = key_rows.reshape(tokens, 2, 128).transpose(1, 0, 2)
    v_in = value_rows.T.reshape(2, 128, tokens)
    f_in = jnp.pad(forget_sums.T.reshape(2, 2, tokens), ((0, 0), (0, 6), (0, 0)))
    bf16, f32 = jnp.bfloat16, jnp.float32
    anywhere = pl.BlockSpec(memory_space=pl.ANY)
    vmem = pl.BlockSpec(memory_space=pltpu.VMEM)
    dma = pltpu.SemaphoreType.DMA
    return pl.pallas_call(
        attention_kernel,
        out_shape=(
            jax.ShapeDtypeStruct((rows, width), bf16),
            jax.ShapeDtypeStruct((rows, width), bf16),
        ),
        in_specs=[anywhere] * 5 + [vmem] * 2,
        out_specs=(vmem, vmem),
        scratch_shapes=[
            pltpu.VMEM((8, 256, 256), bf16),
            pltpu.VMEM((8, 8, 256), f32),
            pltpu.VMEM((8, 2, 256, 128), bf16),
            pltpu.VMEM((8, 2, 128, 256), bf16),
            pltpu.VMEM((8, 2, 8, 256), f32),
            pltpu.VMEM((2, 256, 128), f32),
            pltpu.VMEM((8, 2, 128, 256), f32),
            pltpu.VMEM((8, 8, 256), f32),
            pltpu.VMEM((8, 256, 256), bf16),
            pltpu.VMEM((8, 2, 8, 128), f32),
            pltpu.VMEM((4, 64, 2048), bf16),
            pltpu.VMEM((4, 8, 8, 128), f32),
            pltpu.VMEM((4, 128, 128), f32),
            pltpu.VMEM((64, 2048), bf16),
            pltpu.VMEM((4, 512, 2048), bf16),
            dma((2, 8)),
            dma((2, 8)),
            dma((3, 8, 2)),
            dma((3, 8, 2)),
            dma((8, 4)),
            dma((8, 4)),
            dma((8, 4)),
            dma((8, 4)),
            dma((6,)),
            dma((6,)),
            dma((3,)),
            dma((3,)),
            dma((8,)),
        ],
        compiler_params=pltpu.CompilerParams(
            collective_id=0, has_side_effects=True, vmem_limit_bytes=48 * 1024 * 1024
        ),
        cost_estimate=pl.CostEstimate(
            flops=8 * 10**9, bytes_accessed=16 * 2**20, transcendentals=16 * 2**20
        ),
    )(q_in, k_in, v_in, f_in, out_weight, residual, norm_gain.reshape(1, width))


def local(
    residual,
    queries,
    key_rows,
    value_rows,
    forget_sums,
    out_weight,
    norm_gain,
    expert_ids,
    route_weights,
    expert_gate,
    expert_up,
    expert_down,
    shared_gate,
    shared_up,
    shared_down,
):
    stream, normed = attention(
        residual, queries, key_rows, value_rows, forget_sums, out_weight, norm_gain
    )
    sp_count = lax.axis_size("sp")
    rows_out = normed.shape[0]
    wide = stream.astype(jnp.float32)
    width = normed.shape[1]
    experts_here = expert_gate.shape[0]
    total_experts = experts_here * sp_count
    capacity = 2 * rows_out * TOPK // total_experts
    flat_ids = expert_ids.reshape(-1)
    assigned = flat_ids.shape[0]
    onehot = (flat_ids[:, None] == jnp.arange(total_experts, dtype=jnp.int32)[None, :]).astype(
        jnp.int32
    )
    slot_rank = jnp.sum((jnp.cumsum(onehot, axis=0) - 1) * onehot, axis=1)
    target = flat_ids * capacity + slot_rank
    slot_count = total_experts * capacity
    source = (
        jnp.full((slot_count,), assigned, jnp.int32)
        .at[target]
        .set(jnp.arange(assigned, dtype=jnp.int32))
    )
    padded = jnp.concatenate([normed, jnp.zeros((1, width), jnp.bfloat16)], axis=0)
    outgoing = padded[source // TOPK].reshape(sp_count, experts_here, capacity, width)
    arrived = lax.all_to_all(outgoing, "sp", split_axis=0, concat_axis=0, tiled=True)
    gate_part = jnp.einsum(
        "necd,edf->necf", arrived, expert_gate, preferred_element_type=jnp.float32
    )
    up_part = jnp.einsum("necd,edf->necf", arrived, expert_up, preferred_element_type=jnp.float32)
    hidden = (jax.nn.silu(gate_part) * up_part).astype(jnp.bfloat16)
    processed = jnp.einsum(
        "necf,efd->necd", hidden, expert_down, preferred_element_type=jnp.float32
    ).astype(jnp.bfloat16)
    returned = lax.all_to_all(processed, "sp", split_axis=0, concat_axis=0, tiled=True)
    results = returned.reshape(slot_count, width)
    picked = results[target].reshape(rows_out, TOPK, width).astype(jnp.float32)
    gates = route_weights / jnp.sum(route_weights, axis=1, keepdims=True) * routed_scale
    routed = jnp.sum(gates[:, :, None] * picked, axis=1)
    shared_hidden = (
        jax.nn.silu(jnp.dot(normed, shared_gate, preferred_element_type=jnp.float32))
        * jnp.dot(normed, shared_up, preferred_element_type=jnp.float32)
    ).astype(jnp.bfloat16)
    shared_out = jnp.dot(shared_hidden, shared_down, preferred_element_type=jnp.float32)
    return (wide + shared_out + routed).astype(jnp.bfloat16)


def solution(mesh):
    in_specs = (
        P(("sp", "tp"), None),
        P("sp", "tp"),
        P("sp", "tp"),
        P("sp", "tp"),
        P("sp", "tp"),
        P("tp", None),
        P(),
        P(("sp", "tp"), None),
        P(("sp", "tp"), None),
        P("sp", None, None),
        P("sp", None, None),
        P("sp", None, None),
        P(),
        P(),
        P(),
    )
    out_specs = P(("sp", "tp"), None)
    return jax.shard_map(local, mesh=mesh, in_specs=in_specs, out_specs=out_specs, check_vma=False)
```

```python
import jax
import jax.numpy as jnp
from jax import lax
from jax.experimental import pallas as pl
from jax.experimental.pallas import tpu as pltpu
from jax.sharding import PartitionSpec as P

HEADS = 16
KV_HEADS = 8
HEAD_DIM = 128
TOPK = 4
MESH = pl.DeviceIdType.MESH
LOG2E = 1.4426950408889634
NEG = -1e30

routed_scale = 2.5
norm_eps = 1e-06

NZ, NY, NX = 8, 4, 4
UP_STEPS, DOWN_STEPS = 4, 3


def attention_kernel(
    q_in,
    k_in,
    v_in,
    f_in,
    w_in,
    res_ref,
    gain_ref,
    stream_ref,
    normed_ref,
    qbuf,
    fqbuf,
    kbuf,
    vbuf,
    fbuf,
    bias,
    acc,
    stats,
    obuf,
    lbuf,
    rbuf,
    lrecv,
    wcols,
    att,
    wbuf,
    q_send,
    q_recv,
    kv_send,
    kv_recv,
    o_send,
    o_recv,
    l_send,
    l_recv,
    w_send,
    w_recv,
    p_send,
    p_recv,
    local_sem,
):
    sp = lax.axis_index("sp")
    x = lax.axis_index("tp")
    z = sp // 8
    me8 = sp % 8
    y = me8 // 2
    c = me8 % 2
    zbase = z * 8

    def at_z(step, core):
        return ((z + step + NZ) % NZ) * 8 + y * 2 + core

    partner = zbase + y * 2 + (1 - c)
    xr = (x + 1) % NX
    xl = (x + NX - 1) % NX

    barrier = pltpu.get_barrier_semaphore()

    def greet_plane(i, _):
        n = i + 1
        r8, rx = n // NX, n % NX
        pl.semaphore_signal(
            barrier,
            inc=1,
            device_id=(zbase + (me8 + r8) % 8, (x + rx) % NX),
            device_id_type=MESH,
        )
        return 0

    lax.fori_loop(0, 31, greet_plane, 0)
    for step in (1, -1):
        for core in (0, 1):
            pl.semaphore_signal(
                barrier, inc=1, device_id=(at_z(step, core), x), device_id_type=MESH
            )
    pl.semaphore_wait(barrier, 35)

    def remote(src, dst, send, recv, sp_id, tp_id):
        return pltpu.make_async_remote_copy(
            src_ref=src,
            dst_ref=dst,
            send_sem=send,
            recv_sem=recv,
            device_id=(sp_id, tp_id),
            device_id_type=MESH,
        )

    kv_arrays = ((k_in, kbuf), (v_in, vbuf), (f_in, fbuf))
    first_sends = []
    for a in (2, 0, 1):
        src, dst = kv_arrays[a]
        pltpu.make_async_copy(src.at[c], dst.at[0, c], local_sem.at[a]).start()
        first_sends.append(
            remote(
                src.at[1 - c],
                dst.at[0, c],
                kv_send.at[a, 0, 0],
                kv_recv.at[a, 0, 0],
                partner,
                x,
            )
        )
        for step, slot in ((1, 1), (-1, 1 + UP_STEPS)):
            for h in (0, 1):
                first_sends.append(
                    remote(
                        src.at[h],
                        dst.at[slot, c],
                        kv_send.at[a, slot, h],
                        kv_recv.at[a, slot, c],
                        at_z(step, h),
                        x,
                    )
                )
    for copy in first_sends:
        copy.start()

    pltpu.make_async_copy(q_in.at[c], qbuf.at[me8], local_sem.at[3]).start()
    pltpu.make_async_copy(f_in.at[c], fqbuf.at[me8], local_sem.at[4]).start()
    pltpu.make_async_copy(w_in, wbuf.at[x], local_sem.at[5]).start()

    def q_copies(r):
        to = (me8 + r) % 8
        return (
            remote(f_in.at[to % 2], fqbuf.at[me8], q_send.at[1, r], q_recv.at[1, r], zbase + to, x),
            remote(q_in.at[to % 2], qbuf.at[me8], q_send.at[0, r], q_recv.at[0, r], zbase + to, x),
        )

    def start_q(i, _):
        for copy in q_copies(i + 1):
            copy.start()
        return 0

    lax.fori_loop(0, 7, start_q, 0)

    quarter = w_in.shape[0] // 4
    rows_a = pl.ds(c * 2 * quarter, quarter)
    rows_b = pl.ds(c * 2 * quarter + quarter, quarter)
    rows_half = pl.ds(c * 2 * quarter, 2 * quarter)
    across = (x + 2) % NX
    w_first = [
        remote(w_in.at[rows_a], wbuf.at[x, rows_a], w_send.at[0], w_recv.at[0], sp, xr),
        remote(w_in.at[rows_b], wbuf.at[x, rows_b], w_send.at[2], w_recv.at[2], sp, xl),
        remote(w_in.at[rows_b], wbuf.at[x, rows_b], w_send.at[1], w_recv.at[1], sp, xr),
        remote(w_in.at[rows_a], wbuf.at[x, rows_a], w_send.at[3], w_recv.at[3], sp, xl),
    ]
    for copy in w_first:
        copy.start()
    w_forward = [
        remote(wbuf.at[xl, rows_a], wbuf.at[xl, rows_a], w_send.at[4], w_recv.at[4], sp, xr),
        remote(wbuf.at[xr, rows_b], wbuf.at[xr, rows_b], w_send.at[5], w_recv.at[5], sp, xl),
    ]
    w_partner = [
        remote(wbuf.at[o, rows_half], wbuf.at[o, rows_half], p_send.at[i], p_recv.at[i], partner, x)
        for i, o in enumerate((xl, xr, across))
    ]

    acc[...] = jnp.zeros_like(acc)
    row = lax.broadcasted_iota(jnp.int32, stats.shape, 1)
    stats[...] = jnp.where(row < 2, NEG, 0.0)

    scale = HEAD_DIM ** (-0.5) * LOG2E

    def make_bias(slot):
        f0 = fbuf[slot, 0]
        base = f0[:, 0:1]
        for cc in (0, 1):
            f = f0 if cc == 0 else fbuf[slot, 1]
            b = (base - f) * LOG2E
            bias[cc] = jnp.concatenate([b] * 16, axis=0).T

    def task(slot, qb, masked):
        if masked:
            rows = lax.broadcasted_iota(jnp.int32, (256, 256), 0)
            cols = lax.broadcasted_iota(jnp.int32, (256, 256), 1)
            gap = (qb - 2 * y) * 256
        for h in (0, 1):
            q_h = qbuf[qb, h * 128 : (h + 1) * 128, :]
            delta = (fqbuf[qb, h : h + 1, 0:1] - fbuf[slot, 0, h : h + 1, 0:1]) * LOG2E
            scores = []
            for cc in (0, 1):
                s = jnp.dot(kbuf[slot, cc], q_h, preferred_element_type=jnp.float32)
                s = s * scale + bias[cc, :, h : h + 1]
                if masked:
                    s = jnp.where(rows + cc * 256 <= cols + gap, s, -jnp.inf)
                scores.append(s)
            top = jnp.max(jnp.maximum(scores[0], scores[1]), axis=0, keepdims=True)
            old = stats[qb, h : h + 1, :]
            new = jnp.maximum(old, top + delta)
            shift = new - delta
            factor = jnp.exp2(old - new)
            p = [jnp.exp2(s - shift) for s in scores]
            total = jnp.sum(p[0] + p[1], axis=0, keepdims=True)
            stats[qb, h : h + 1, :] = new
            stats[qb, 2 + h : 3 + h, :] = stats[qb, 2 + h : 3 + h, :] * factor + total
            mixed = jnp.dot(
                vbuf[slot, 0], p[0].astype(jnp.bfloat16), preferred_element_type=jnp.float32
            ) + jnp.dot(
                vbuf[slot, 1], p[1].astype(jnp.bfloat16), preferred_element_type=jnp.float32
            )
            acc[qb, h] = acc[qb, h] * factor + mixed

    def wait_first(a, slot):
        for h in (0, 1):
            remote(
                kv_arrays[a][0].at[h],
                kv_arrays[a][1].at[slot, h],
                kv_send.at[a, slot, h],
                kv_recv.at[a, slot, h],
                partner,
                x,
            ).wait_recv()

    def forward(a, slot, step):
        buf = kv_arrays[a][1]
        return remote(
            buf.at[slot],
            buf.at[slot + 1],
            kv_send.at[a, slot + 1, 0],
            kv_recv.at[a, slot + 1, 0],
            at_z(step, c),
            x,
        )

    forwards = []

    def arrive(slot, step, first, send_on):
        for a in (2, 0, 1):
            if first:
                wait_first(a, slot)
            else:
                forward(a, slot - 1, step).wait_recv()
            if send_on:
                copy = forward(a, slot, step)
                copy.start()
                forwards.append(copy)

    def absorb(slot, origin_ok):
        @pl.when(origin_ok)
        def _():
            make_bias(slot)

            def body(qb, _):
                task(slot, qb, False)
                return 0

            lax.fori_loop(0, 8, body, 0)

    for a in range(3):
        pltpu.make_async_copy(
            kv_arrays[a][0].at[c], kv_arrays[a][1].at[0, c], local_sem.at[a]
        ).wait()
        remote(
            kv_arrays[a][0].at[1 - c],
            kv_arrays[a][1].at[0, c],
            kv_send.at[a, 0, 0],
            kv_recv.at[a, 0, 0],
            partner,
            x,
        ).wait_recv()
    pltpu.make_async_copy(q_in.at[c], qbuf.at[me8], local_sem.at[3]).wait()
    pltpu.make_async_copy(f_in.at[c], fqbuf.at[me8], local_sem.at[4]).wait()
    arrive(1, 1, True, True)
    arrive(1 + UP_STEPS, -1, True, True)
    make_bias(0)

    def own(r, _):
        @pl.when(r > 0)
        def _():
            for copy in q_copies(jnp.maximum(r, 1)):
                copy.wait_recv()

        qb = (me8 + 8 - r) % 8

        @pl.when(qb // 2 >= y)
        def _():
            task(0, qb, True)

        return 0

    lax.fori_loop(0, 8, own, 0)
    w_first[0].wait_recv()
    w_forward[0].start()
    w_first[2 - 1].wait_recv()
    w_forward[1].start()
    absorb(1, z >= 1)
    absorb(5, z + 1 >= NZ)
    arrive(2, 1, False, True)
    arrive(6, -1, False, True)
    absorb(2, z >= 2)
    absorb(6, z + 2 >= NZ)
    arrive(3, 1, False, True)
    arrive(7, -1, False, False)
    w_first[2].wait_recv()
    w_partner[0].start()
    w_first[3].wait_recv()
    w_partner[1].start()
    absorb(3, z >= 3)
    absorb(7, z + 3 >= NZ)
    arrive(4, 1, False, False)
    absorb(4, z >= 4)
    w_forward[0].wait_recv()
    w_forward[1].wait_recv()
    w_partner[2].start()

    def o_copy(r8, rx):
        to = (me8 + r8) % 8
        tx = (x + rx) % NX
        return (
            remote(
                obuf.at[to, pl.ds(tx * 64, 64)],
                rbuf.at[y, :, pl.ds((x * 2 + c) * 256, 256)],
                o_send.at[r8, rx],
                o_recv.at[r8, rx],
                zbase + to,
                tx,
            ),
            remote(
                lbuf.at[to, tx // 2],
                lrecv.at[y, x * 2 + c],
                l_send.at[r8, rx],
                l_recv.at[r8, rx],
                zbase + to,
                tx,
            ),
        )

    def finish(r, _):
        r8 = 7 - r
        qb = (me8 + r8) % 8
        sums = []
        for h in (0, 1):
            total = stats[qb, 2 + h : 3 + h, :]
            some = total > 0.0
            inv = jnp.where(some, 1.0 / jnp.where(some, total, 1.0), 0.0)
            obuf[qb, :, h * 128 : (h + 1) * 128] = (acc[qb, h] * inv).T.astype(jnp.bfloat16)
            sums.append(
                jnp.where(
                    some, stats[qb, h : h + 1, :] + jnp.log2(jnp.where(some, total, 1.0)), NEG
                )
            )
        both = jnp.concatenate(sums + [jnp.zeros((6, 256), jnp.float32)], axis=0)
        lbuf[qb, 0] = both[:, :128]
        lbuf[qb, 1] = both[:, 128:]
        for rx in (2, 1, 3):
            for copy in o_copy(r8, rx):
                copy.start()

        @pl.when(r8 > 0)
        def _():
            for copy in o_copy(r8, 0):
                copy.start()

        return 0

    lax.fori_loop(0, 8, finish, 0)
    own_copies = (
        pltpu.make_async_copy(
            obuf.at[me8, pl.ds(x * 64, 64)],
            rbuf.at[y, :, pl.ds((x * 2 + c) * 256, 256)],
            local_sem.at[6],
        ),
        pltpu.make_async_copy(lbuf.at[me8, x // 2], lrecv.at[y, x * 2 + c], local_sem.at[7]),
    )
    for copy in own_copies:
        copy.start()
    for copy in own_copies:
        copy.wait()

    def wait_o(r, _):
        for copy in o_copy((r + 1) // NX, (r + 1) % NX):
            copy.wait_recv()
        return 0

    lax.fori_loop(0, 31, wait_o, 0)

    logs = [lrecv[i].reshape(64, 128) for i in range(NY)]
    top = jnp.maximum(jnp.maximum(logs[0], logs[1]), jnp.maximum(logs[2], logs[3]))
    parts = [jnp.exp2(v - top) for v in logs]
    inv = 1.0 / (parts[0] + parts[1] + parts[2] + parts[3])
    for i in range(NY):
        scaled = parts[i] * inv
        wcols[i] = jnp.concatenate([scaled, scaled], axis=0).T
    first_row = pl.multiple_of((x % 2) * 64, 64)
    shares = [wcols[i, pl.ds(first_row, 64), :] for i in range(NY)]
    for n in range(HEADS):
        lane = (n // 2) * 8 + n % 2
        cols = slice(n * 128, (n + 1) * 128)
        mixed = shares[0][:, lane : lane + 1] * rbuf[0, :, cols].astype(jnp.float32)
        for i in range(1, NY):
            mixed = mixed + shares[i][:, lane : lane + 1] * rbuf[i, :, cols].astype(jnp.float32)
        att[:, cols] = mixed.astype(jnp.bfloat16)

    pltpu.make_async_copy(w_in, wbuf.at[x], local_sem.at[5]).wait()
    for copy in w_partner:
        copy.wait_recv()

    width = w_in.shape[1]
    chunk = 256

    def project(i, total):
        cols = pl.ds(pl.multiple_of(i * chunk, chunk), chunk)
        part = jnp.dot(att[:, 0:512], wbuf[0, :, cols], preferred_element_type=jnp.float32)
        for b in range(1, NX):
            part = part + jnp.dot(
                att[:, b * 512 : (b + 1) * 512],
                wbuf[b, :, cols],
                preferred_element_type=jnp.float32,
            )
        stream = (res_ref[:, cols].astype(jnp.float32) + part).astype(jnp.bfloat16)
        stream_ref[:, cols] = stream
        wide = stream.astype(jnp.float32)
        return total + jnp.sum(wide * wide, axis=1, keepdims=True)

    total = lax.fori_loop(0, width // chunk, project, jnp.zeros((64, 1), jnp.float32))
    rate = lax.rsqrt(total * (1.0 / width) + norm_eps)
    normed_ref[...] = (stream_ref[...].astype(jnp.float32) * rate * gain_ref[...]).astype(
        jnp.bfloat16
    )

    for copy in first_sends + forwards + w_first + w_forward + w_partner:
        copy.wait_send()

    def wait_q(i, _):
        for copy in q_copies(i + 1):
            copy.wait_send()
        return 0

    lax.fori_loop(0, 7, wait_q, 0)

    def wait_sent(r, _):
        for copy in o_copy((r + 1) // NX, (r + 1) % NX):
            copy.wait_send()
        return 0

    lax.fori_loop(0, 31, wait_sent, 0)


def attention(residual, queries, key_rows, value_rows, forget_sums, out_weight, norm_gain):
    rows, width = residual.shape
    tokens = queries.shape[0]
    q_in = queries.T.reshape(2, 256, tokens)
    k_in = key_rows.reshape(tokens, 2, 128).transpose(1, 0, 2)
    v_in = value_rows.T.reshape(2, 128, tokens)
    f_in = jnp.pad(forget_sums.T.reshape(2, 2, tokens), ((0, 0), (0, 6), (0, 0)))
    bf16, f32 = jnp.bfloat16, jnp.float32
    anywhere = pl.BlockSpec(memory_space=pl.ANY)
    vmem = pl.BlockSpec(memory_space=pltpu.VMEM)
    dma = pltpu.SemaphoreType.DMA
    return pl.pallas_call(
        attention_kernel,
        out_shape=(
            jax.ShapeDtypeStruct((rows, width), bf16),
            jax.ShapeDtypeStruct((rows, width), bf16),
        ),
        in_specs=[anywhere] * 5 + [vmem] * 2,
        out_specs=(vmem, vmem),
        scratch_shapes=[
            pltpu.VMEM((8, 256, 256), bf16),
            pltpu.VMEM((8, 8, 256), f32),
            pltpu.VMEM((8, 2, 256, 128), bf16),
            pltpu.VMEM((8, 2, 128, 256), bf16),
            pltpu.VMEM((8, 2, 8, 256), f32),
            pltpu.VMEM((2, 256, 128), f32),
            pltpu.VMEM((8, 2, 128, 256), f32),
            pltpu.VMEM((8, 8, 256), f32),
            pltpu.VMEM((8, 256, 256), bf16),
            pltpu.VMEM((8, 2, 8, 128), f32),
            pltpu.VMEM((4, 64, 2048), bf16),
            pltpu.VMEM((4, 8, 8, 128), f32),
            pltpu.VMEM((4, 128, 128), f32),
            pltpu.VMEM((64, 2048), bf16),
            pltpu.VMEM((4, 512, 2048), bf16),
            dma((2, 8)),
            dma((2, 8)),
            dma((3, 8, 2)),
            dma((3, 8, 2)),
            dma((8, 4)),
            dma((8, 4)),
            dma((8, 4)),
            dma((8, 4)),
            dma((6,)),
            dma((6,)),
            dma((3,)),
            dma((3,)),
            dma((8,)),
        ],
        compiler_params=pltpu.CompilerParams(
            collective_id=0, has_side_effects=True, vmem_limit_bytes=48 * 1024 * 1024
        ),
        cost_estimate=pl.CostEstimate(
            flops=8 * 10**9, bytes_accessed=16 * 2**20, transcendentals=16 * 2**20
        ),
    )(q_in, k_in, v_in, f_in, out_weight, residual, norm_gain.reshape(1, width))


def experts_kernel(
    normed_ref,
    stream_ref,
    ids_ref,
    route_ref,
    eg_in,
    eu_in,
    ed_in,
    sg_in,
    su_in,
    sd_in,
    out_ref,
    nbuf,
    table,
    tables,
    sel,
    gate,
    sbuf,
    xbuf,
    obuf,
    rbuf,
    cin,
    cout,
    total,
    eg,
    eu,
    ed,
    sg,
    su,
    sd,
    n_send,
    n_recv,
    t_send,
    t_recv,
    x_send,
    x_recv,
    r_send,
    r_recv,
    c_send,
    c_recv,
    w_sem,
    x_sem,
    r_sem,
):
    sp = lax.axis_index("sp")
    x = lax.axis_index("tp")
    z = sp // 8
    me8 = sp % 8
    zbase = z * 8
    width = normed_ref.shape[1]
    half = width // 2

    def at_z(step):
        return ((z + step + NZ) % NZ) * 8 + me8

    barrier = pltpu.get_barrier_semaphore()
    for r in range(1, 8):
        for to in (zbase + (me8 + r) % 8, at_z(r)):
            pl.semaphore_signal(barrier, inc=1, device_id=(to, x), device_id_type=MESH)
    loads = [
        pltpu.make_async_copy(src, dst, w_sem.at[i])
        for i, (src, dst) in enumerate(
            (
                (sg_in, sg),
                (su_in, su),
                (sd_in, sd),
                (eg_in.at[0], eg),
                (eu_in.at[0], eu),
                (ed_in.at[0], ed),
            )
        )
    ]
    for copy in loads:
        copy.start()
    nbuf[0, 0] = normed_ref[:, :half]
    nbuf[0, 1] = normed_ref[:, half:]
    pl.semaphore_wait(barrier, 14)

    def remote(src, dst, send, recv, sp_id):
        return pltpu.make_async_remote_copy(
            src_ref=src,
            dst_ref=dst,
            send_sem=send,
            recv_sem=recv,
            device_id=(sp_id, x),
            device_id_type=MESH,
        )

    def pass_on(slot, to_slot, hf, step):
        return remote(
            nbuf.at[slot, hf],
            nbuf.at[to_slot, hf],
            n_send.at[to_slot, hf],
            n_recv.at[to_slot, hf],
            at_z(step),
        )

    sent = []

    def send(copy):
        copy.start()
        sent.append(copy)

    up, down = 1, 1 + UP_STEPS
    for hf in (0, 1):
        send(pass_on(0, up, hf, 1))
        send(pass_on(0, down, hf, -1))

    f32, bf16 = jnp.float32, jnp.bfloat16
    ids = ids_ref[...]
    weights = route_ref[...]
    gates = weights / jnp.sum(weights, axis=1, keepdims=True) * routed_scale
    rows = ids.shape[0]
    experts = lax.broadcasted_iota(jnp.int32, (rows, 64), 1)
    named = jnp.zeros((rows, 64), f32)
    shares = jnp.zeros((rows, 64), f32)
    for k in range(TOPK):
        hit = ids[:, k : k + 1] == experts
        named = named + jnp.where(hit, 1.0, 0.0)
        shares = shares + jnp.where(hit, gates[:, k : k + 1], 0.0)
    earlier = (
        lax.broadcasted_iota(jnp.int32, (rows, rows), 1)
        < lax.broadcasted_iota(jnp.int32, (rows, rows), 0)
    )
    named = named.astype(bf16)
    rank = jnp.dot(jnp.where(earlier, 1.0, 0.0).astype(bf16), named, preferred_element_type=f32)
    lane = lax.broadcasted_iota(jnp.int32, (64, 1024), 1)
    expert = lax.broadcasted_iota(jnp.int32, (64, 1024), 0)
    spread = jnp.where(lane // 16 == expert, 1.0, 0.0).astype(bf16)
    named_x = jnp.dot(named, spread, preferred_element_type=f32)
    rank_x = jnp.dot(rank.astype(bf16), spread, preferred_element_type=f32)
    share_x = jnp.dot(shares.astype(bf16), spread, preferred_element_type=f32)
    want = (lax.broadcasted_iota(jnp.int32, (rows, 1024), 1) % 8).astype(f32)
    filled = jnp.where(rank_x == want, named_x, 0.0)
    token = lax.broadcasted_iota(jnp.int32, (rows, 1024), 0).astype(f32)
    source = jnp.sum(filled * (token + 1000.0), axis=0, keepdims=True) - 1000.0
    share = jnp.sum(filled * share_x, axis=0, keepdims=True)
    for p in range(NZ):
        lanes = slice(p * 128, (p + 1) * 128)
        table[p] = jnp.concatenate(
            [source[:, lanes], share[:, lanes], jnp.zeros((6, 128), f32)], axis=0
        )
    tables[z] = table[z]

    def table_copy(r):
        to = (z + r) % NZ
        return remote(table.at[to], tables.at[z], t_send.at[r], t_recv.at[r], to * 8 + me8)

    for r in range(1, NZ):
        send(table_copy(r))

    for copy in loads[:3]:
        copy.wait()
    n = normed_ref[...]
    g = jnp.dot(n, sg[...], preferred_element_type=f32)
    u = jnp.dot(n, su[...], preferred_element_type=f32)
    hidden = (g / (1.0 + jnp.exp(-g)) * u).astype(bf16)
    for i in range(4):
        cols = slice(i * width // 4, (i + 1) * width // 4)
        total[:, cols] = stream_ref[:, cols].astype(f32) + jnp.dot(
            hidden, sd[:, cols], preferred_element_type=f32
        )

    pairs = ((1, 5), (2, 6), (3, 7), (4, 0))
    offset = {0: 0, 1: -1, 2: -2, 3: -3, 4: -4, 5: 1, 6: 2, 7: 3}

    def arrive(slot, step, send_on):
        for hf in (0, 1):
            pass_on(slot - 1 if slot not in (up, down) else 0, slot, hf, step).wait_recv()
            if send_on:
                send(pass_on(slot, slot + 1, hf, step))

    def x_copy(b, r):
        to = (me8 + r) % 8
        return remote(sbuf.at[b, to], xbuf.at[b, me8], x_send.at[b, r], x_recv.at[b, r], zbase + to)

    def r_copy(b, r):
        to = (me8 + r) % 8
        return remote(obuf.at[b, to], rbuf.at[b, me8], r_send.at[b, r], r_recv.at[b, r], zbase + to)

    def x_own(b):
        return pltpu.make_async_copy(sbuf.at[b, me8], xbuf.at[b, me8], x_sem.at[b])

    def r_own(b):
        return pltpu.make_async_copy(obuf.at[b, me8], rbuf.at[b, me8], r_sem.at[b])

    def dispatch(b):
        first, second = pairs[b]
        ta = tables[(z + offset[first] + NZ) % NZ]
        tb = tables[(z + offset[second] + NZ) % NZ]
        lane_of = lax.broadcasted_iota(jnp.int32, (1, 128), 1) % 16
        src = jnp.where(lane_of < 8, ta[0:1], tb[0:1] + 64.0)
        share_row = jnp.where(lane_of < 8, ta[1:2], tb[1:2])
        token_of = lax.broadcasted_iota(jnp.int32, (128, 128), 0).astype(f32)
        chosen = jnp.where(token_of == src, 1.0, 0.0)
        sel[...] = chosen.T.astype(bf16)
        gate[b] = (chosen * share_row).astype(bf16)
        for hf in (0, 1):
            for i in range(2):
                cols = slice(i * half // 2, (i + 1) * half // 2)
                tokens = jnp.concatenate([nbuf[first, hf, :, cols], nbuf[second, hf, :, cols]], axis=0)
                picked = jnp.dot(sel[...], tokens, preferred_element_type=f32)
                at = hf * half + i * half // 2
                sbuf[b, :, :, at : at + half // 2] = picked.astype(bf16).reshape(8, 16, half // 2)
        for r in (4, 3, 5, 2, 6, 1, 7):
            send(x_copy(b, r))
        x_own(b).start()

    def run_expert(b):
        for r in range(1, 8):
            x_copy(b, r).wait_recv()
        x_own(b).wait()
        rows_in = xbuf[b].reshape(128, width)
        g = jnp.dot(rows_in, eg[...], preferred_element_type=f32)
        u = jnp.dot(rows_in, eu[...], preferred_element_type=f32)
        hidden = (g / (1.0 + jnp.exp(-g)) * u).astype(bf16)
        for i in range(4):
            cols = slice(i * width // 4, (i + 1) * width // 4)
            made = jnp.dot(hidden, ed[:, cols], preferred_element_type=f32)
            obuf[b, :, :, cols] = made.astype(bf16).reshape(8, 16, width // 4)

    def give_back(b):
        for r in (4, 3, 5, 2, 6, 1, 7):
            send(r_copy(b, r))
        r_own(b).start()

    def need_tables(*steps):
        for r in steps:
            table_copy(r).wait_recv()

    arrive(1, 1, True)
    arrive(5, -1, True)
    need_tables(1, 7)
    dispatch(0)
    for copy in loads[3:]:
        copy.wait()
    arrive(2, 1, True)
    arrive(6, -1, True)
    need_tables(2, 6)
    dispatch(1)
    run_expert(0)
    arrive(3, 1, True)
    arrive(7, -1, False)
    need_tables(3, 5)
    dispatch(2)
    run_expert(1)
    arrive(4, 1, False)
    need_tables(4)
    dispatch(3)
    run_expert(2)
    give_back(2)
    run_expert(3)
    give_back(3)
    give_back(1)
    give_back(0)

    def chain_copy(way, place, hf):
        return remote(
            cout.at[way, place, hf],
            cin.at[way, place, hf],
            c_send.at[way, place, hf],
            c_recv.at[way, place, hf],
            at_z(-1 if way == 0 else 1),
        )

    for b, places in ((3, (3, None)), (2, (2, 2)), (1, (1, 1)), (0, (0, 0))):
        for r in range(1, 8):
            r_copy(b, r).wait_recv()
        r_own(b).wait()
        for hf in (0, 1):
            cols = slice(hf * half, (hf + 1) * half)
            part = jnp.dot(
                gate[b], rbuf[b, :, :, cols].reshape(128, half), preferred_element_type=f32
            )
            for way in (0, 1):
                mine = part[way * 64 : (way + 1) * 64]
                place = places[way]
                if place is None:
                    total[:, cols] = total[:, cols] + mine
                    continue
                if place < (3 if way == 0 else 2):
                    chain_copy(way, place + 1, hf).wait_recv()
                    mine = mine + cin[way, place + 1, hf].astype(f32)
                cout[way, place, hf] = mine.astype(bf16)
                send(chain_copy(way, place, hf))
    for hf in (0, 1):
        cols = slice(hf * half, (hf + 1) * half)
        for way in (0, 1):
            chain_copy(way, 0, hf).wait_recv()
        out_ref[:, cols] = (
            total[:, cols] + cin[0, 0, hf].astype(f32) + cin[1, 0, hf].astype(f32)
        ).astype(bf16)
    for copy in sent:
        copy.wait_send()


def experts(
    normed,
    stream,
    expert_ids,
    route_weights,
    expert_gate,
    expert_up,
    expert_down,
    shared_gate,
    shared_up,
    shared_down,
):
    rows, width = normed.shape
    hidden = expert_gate.shape[2]
    shared = shared_gate.shape[1]
    bf16, f32 = jnp.bfloat16, jnp.float32
    anywhere = pl.BlockSpec(memory_space=pl.ANY)
    vmem = pl.BlockSpec(memory_space=pltpu.VMEM)
    dma = pltpu.SemaphoreType.DMA
    return pl.pallas_call(
        experts_kernel,
        out_shape=jax.ShapeDtypeStruct((rows, width), bf16),
        in_specs=[vmem] * 4 + [anywhere] * 6,
        out_specs=vmem,
        scratch_shapes=[
            pltpu.VMEM((8, 2, rows, width // 2), bf16),
            pltpu.VMEM((8, 8, 128), f32),
            pltpu.VMEM((8, 8, 128), f32),
            pltpu.VMEM((128, 128), bf16),
            pltpu.VMEM((4, 128, 128), bf16),
            pltpu.VMEM((4, 8, 16, width), bf16),
            pltpu.VMEM((4, 8, 16, width), bf16),
            pltpu.VMEM((4, 8, 16, width), bf16),
            pltpu.VMEM((4, 8, 16, width), bf16),
            pltpu.VMEM((2, 4, 2, rows, width // 2), bf16),
            pltpu.VMEM((2, 4, 2, rows, width // 2), bf16),
            pltpu.VMEM((rows, width), f32),
            pltpu.VMEM((width, hidden), bf16),
            pltpu.VMEM((width, hidden), bf16),
            pltpu.VMEM((hidden, width), bf16),
            pltpu.VMEM((width, shared), bf16),
            pltpu.VMEM((width, shared), bf16),
            pltpu.VMEM((shared, width), bf16),
            dma((8, 2)),
            dma((8, 2)),
            dma((8,)),
            dma((8,)),
            dma((4, 8)),
            dma((4, 8)),
            dma((4, 8)),
            dma((4, 8)),
            dma((2, 4, 2)),
            dma((2, 4, 2)),
            dma((6,)),
            dma((4,)),
            dma((4,)),
        ],
        compiler_params=pltpu.CompilerParams(
            collective_id=1, has_side_effects=True, vmem_limit_bytes=48 * 1024 * 1024
        ),
        cost_estimate=pl.CostEstimate(
            flops=4 * 10**9, bytes_accessed=16 * 2**20, transcendentals=2**20
        ),
    )(
        normed,
        stream,
        expert_ids,
        route_weights,
        expert_gate,
        expert_up,
        expert_down,
        shared_gate,
        shared_up,
        shared_down,
    )


def local(
    residual,
    queries,
    key_rows,
    value_rows,
    forget_sums,
    out_weight,
    norm_gain,
    expert_ids,
    route_weights,
    expert_gate,
    expert_up,
    expert_down,
    shared_gate,
    shared_up,
    shared_down,
):
    stream, normed = attention(
        residual, queries, key_rows, value_rows, forget_sums, out_weight, norm_gain
    )
    return experts(
        normed,
        stream,
        expert_ids,
        route_weights,
        expert_gate,
        expert_up,
        expert_down,
        shared_gate,
        shared_up,
        shared_down,
    )


def solution(mesh):
    in_specs = (
        P(("sp", "tp"), None),
        P("sp", "tp"),
        P("sp", "tp"),
        P("sp", "tp"),
        P("sp", "tp"),
        P("tp", None),
        P(),
        P(("sp", "tp"), None),
        P(("sp", "tp"), None),
        P("sp", None, None),
        P("sp", None, None),
        P("sp", None, None),
        P(),
        P(),
        P(),
    )
    out_specs = P(("sp", "tp"), None)
    return jax.shard_map(local, mesh=mesh, in_specs=in_specs, out_specs=out_specs, check_vma=False)
```

```python
import jax
import jax.numpy as jnp
from jax import lax
from jax.experimental import pallas as pl
from jax.experimental.pallas import tpu as pltpu
from jax.sharding import PartitionSpec as P

HEADS = 16
KV_HEADS = 8
HEAD_DIM = 128
TOPK = 4
MESH = pl.DeviceIdType.MESH
LOG2E = 1.4426950408889634
NEG = -1e30

routed_scale = 2.5
norm_eps = 1e-06

NZ, NY, NX = 8, 4, 4
UP_STEPS, DOWN_STEPS = 4, 3


def attention_kernel(
    q_in,
    k_rows,
    v_in,
    f_rows,
    w_in,
    res_in,
    gain_in,
    stream_ref,
    normed_ref,
    qbuf,
    fqbuf,
    kbuf,
    vbuf,
    fbuf,
    f_in,
    bias,
    ones,
    held_a,
    held_b,
    res_ref,
    gain_ref,
    acc,
    stats,
    obuf,
    lbuf,
    rbuf,
    lrecv,
    wcols,
    att,
    wbuf,
    q_send,
    q_recv,
    kv_send,
    kv_recv,
    o_send,
    o_recv,
    l_send,
    l_recv,
    w_send,
    w_recv,
    p_send,
    p_recv,
    local_sem,
):
    sp = lax.axis_index("sp")
    x = lax.axis_index("tp")
    z = sp // 8
    me8 = sp % 8
    y = me8 // 2
    c = me8 % 2
    zbase = z * 8

    def at_z(step, core):
        return ((z + step + NZ) % NZ) * 8 + y * 2 + core

    partner = zbase + y * 2 + (1 - c)
    xr = (x + 1) % NX
    xl = (x + NX - 1) % NX

    barrier = pltpu.get_barrier_semaphore()

    def greet_plane(i, _):
        n = i + 1
        r8, rx = n // NX, n % NX
        pl.semaphore_signal(
            barrier,
            inc=1,
            device_id=(zbase + (me8 + r8) % 8, (x + rx) % NX),
            device_id_type=MESH,
        )
        return 0

    lax.fori_loop(0, 31, greet_plane, 0)
    for step in (1, -1):
        for core in (0, 1):
            pl.semaphore_signal(
                barrier, inc=1, device_id=(at_z(step, core), x), device_id_type=MESH
            )
    pltpu.make_async_copy(q_in.at[c], qbuf.at[me8], local_sem.at[3]).start()
    pltpu.make_async_copy(w_in, wbuf.at[x], local_sem.at[5]).start()
    pltpu.make_async_copy(res_in, res_ref, local_sem.at[8]).start()
    pltpu.make_async_copy(gain_in, gain_ref, local_sem.at[9]).start()
    for h in (0, 1):
        f_in[h] = jnp.concatenate(
            [f_rows[2 * h : 2 * h + 2, :], jnp.zeros((6, f_rows.shape[1]), jnp.float32)], axis=0
        )
        row = lax.broadcasted_iota(jnp.int32, (128, 256), 0)
        ones[h] = jnp.where((row % 8 == h) & (row < 24), 1.0, 0.0).astype(jnp.bfloat16)
    acc[...] = jnp.zeros_like(acc)
    row = lax.broadcasted_iota(jnp.int32, stats.shape, 1)
    stats[...] = jnp.where(row < 2, NEG, 0.0)
    pl.semaphore_wait(barrier, 35)

    def remote(src, dst, send, recv, sp_id, tp_id):
        return pltpu.make_async_remote_copy(
            src_ref=src,
            dst_ref=dst,
            send_sem=send,
            recv_sem=recv,
            device_id=(sp_id, tp_id),
            device_id_type=MESH,
        )

    kv_arrays = ((k_rows, kbuf), (v_in, vbuf), (f_in, fbuf))

    def own_piece(a, h):
        if a == 0:
            return k_rows.at[:, pl.ds(pl.multiple_of(h * 128, 128), 128)]
        return kv_arrays[a][0].at[h]

    first_sends = []
    for a in (2, 0, 1):
        dst = kv_arrays[a][1]
        pltpu.make_async_copy(own_piece(a, c), dst.at[0, c], local_sem.at[a]).start()
        first_sends.append(
            remote(
                own_piece(a, 1 - c),
                dst.at[0, c],
                kv_send.at[a, 0, 0],
                kv_recv.at[a, 0, 0],
                partner,
                x,
            )
        )
        for step, slot in ((1, 1), (-1, 1 + UP_STEPS)):
            for h in (0, 1):
                first_sends.append(
                    remote(
                        own_piece(a, h),
                        dst.at[slot, c],
                        kv_send.at[a, slot, h],
                        kv_recv.at[a, slot, c],
                        at_z(step, h),
                        x,
                    )
                )
    for copy in first_sends:
        copy.start()

    pltpu.make_async_copy(f_in.at[c], fqbuf.at[me8], local_sem.at[4]).start()

    def q_copies(r):
        to = (me8 + r) % 8
        return (
            remote(f_in.at[to % 2], fqbuf.at[me8], q_send.at[1, r], q_recv.at[1, r], zbase + to, x),
            remote(q_in.at[to % 2], qbuf.at[me8], q_send.at[0, r], q_recv.at[0, r], zbase + to, x),
        )

    def start_q(i, _):
        for copy in q_copies(i + 1):
            copy.start()
        return 0

    lax.fori_loop(0, 7, start_q, 0)

    quarter = w_in.shape[0] // 4
    rows_a = pl.ds(c * 2 * quarter, quarter)
    rows_b = pl.ds(c * 2 * quarter + quarter, quarter)
    rows_half = pl.ds(c * 2 * quarter, 2 * quarter)
    across = (x + 2) % NX
    w_first = [
        remote(w_in.at[rows_a], wbuf.at[x, rows_a], w_send.at[0], w_recv.at[0], sp, xr),
        remote(w_in.at[rows_b], wbuf.at[x, rows_b], w_send.at[2], w_recv.at[2], sp, xl),
        remote(w_in.at[rows_b], wbuf.at[x, rows_b], w_send.at[1], w_recv.at[1], sp, xr),
        remote(w_in.at[rows_a], wbuf.at[x, rows_a], w_send.at[3], w_recv.at[3], sp, xl),
    ]
    for copy in w_first:
        copy.start()
    w_forward = [
        remote(wbuf.at[xl, rows_a], wbuf.at[xl, rows_a], w_send.at[4], w_recv.at[4], sp, xr),
        remote(wbuf.at[xr, rows_b], wbuf.at[xr, rows_b], w_send.at[5], w_recv.at[5], sp, xl),
    ]
    w_partner = [
        remote(wbuf.at[o, rows_half], wbuf.at[o, rows_half], p_send.at[i], p_recv.at[i], partner, x)
        for i, o in enumerate((xl, xr, across))
    ]

    scale = HEAD_DIM ** (-0.5) * LOG2E
    root = HEAD_DIM**0.5

    def make_bias(slot):
        f0 = fbuf[slot, 0]
        base = f0[:, 0:1]
        for cc in (0, 1):
            rest = (base - (f0 if cc == 0 else fbuf[slot, 1])) * root
            pieces = []
            for _ in range(3):
                piece = rest.astype(jnp.bfloat16).astype(jnp.float32)
                pieces.append(piece)
                rest = rest - piece
            pieces.append(jnp.zeros((104, 256), jnp.float32))
            bias[slot, cc] = jnp.concatenate(pieces, axis=0).T.astype(jnp.bfloat16)

    def score(slot, qb, h, cc):
        q_h = jnp.concatenate([qbuf[qb, h * 128 : (h + 1) * 128, :], ones[h]], axis=0)
        keys = jnp.concatenate([kbuf[slot, cc], bias[slot, cc]], axis=1)
        return jnp.dot(keys, q_h, preferred_element_type=jnp.float32)

    span = 64

    def weigh(slot, qb, h, held):
        delta = (fqbuf[qb, h : h + 1, 0:1] - fbuf[slot, 0, h : h + 1, 0:1]) * root
        pieces = [(cc, slice(r, r + span)) for cc in (0, 1) for r in range(0, 256, span)]
        top = None
        for cc, part in pieces:
            high = jnp.max(held[h, cc, part, :].reshape(span // 8, 8, 256), axis=0)
            top = high if top is None else jnp.maximum(top, high)
        top = jnp.max(top, axis=0, keepdims=True)
        old = stats[qb, h : h + 1, :]
        new = jnp.maximum(old, top + delta)
        shift = new - delta
        factor = jnp.exp2((old - new) * scale)
        total = jnp.zeros((8, 256), jnp.float32)
        p = ([], [])
        for cc, part in pieces:
            e = jnp.exp2((held[h, cc, part, :] - shift) * scale)
            total = total + jnp.sum(e.reshape(span // 8, 8, 256), axis=0)
            p[cc].append(e.astype(jnp.bfloat16))
        total = jnp.sum(total, axis=0, keepdims=True)
        stats[qb, h : h + 1, :] = new
        stats[qb, 2 + h : 3 + h, :] = stats[qb, 2 + h : 3 + h, :] * factor + total
        mixed = jnp.dot(
            vbuf[slot, 0], jnp.concatenate(p[0], axis=0), preferred_element_type=jnp.float32
        ) + jnp.dot(vbuf[slot, 1], jnp.concatenate(p[1], axis=0), preferred_element_type=jnp.float32)
        acc[qb, h] = acc[qb, h] * factor + mixed

    def own_task(qb):
        rows = lax.broadcasted_iota(jnp.int32, (256, 256), 0)
        cols = lax.broadcasted_iota(jnp.int32, (256, 256), 1)
        gap = (qb - 2 * y) * 256
        for h in (0, 1):
            for cc in (0, 1):
                held_a[h, cc] = jnp.where(
                    rows + cc * 256 <= cols + gap, score(0, qb, h, cc), -jnp.inf
                )
        use(held_a, 0, qb)

    def fill(held, slot, qb):
        for h in (0, 1):
            for cc in (0, 1):
                held[h, cc] = score(slot, qb, h, cc)

    def use(held, slot, qb):
        for h in (0, 1):
            weigh(slot, qb, h, held)

    def run_tasks(count, place, after=None):
        @pl.when(count > 0)
        def _():
            fill(held_a, *place(0))

        def pair(i, _):
            first, second = 2 * i, 2 * i + 1
            fill(held_b, *place(second))
            use(held_a, *place(first))
            if after is not None:
                after(first)
            fill(held_a, *place(jnp.minimum(second + 1, count - 1)))
            use(held_b, *place(second))
            if after is not None:
                after(second)
            return 0

        lax.fori_loop(0, count // 2, pair, 0)

    def wait_first(a, slot):
        for h in (0, 1):
            remote(
                own_piece(a, h),
                kv_arrays[a][1].at[slot, h],
                kv_send.at[a, slot, h],
                kv_recv.at[a, slot, h],
                partner,
                x,
            ).wait_recv()

    def forward(a, slot, step):
        buf = kv_arrays[a][1]
        return remote(
            buf.at[slot],
            buf.at[slot + 1],
            kv_send.at[a, slot + 1, 0],
            kv_recv.at[a, slot + 1, 0],
            at_z(step, c),
            x,
        )

    forwards = []

    def arrive(slot, step, first, send_on):
        for a in (2, 0, 1):
            if first:
                wait_first(a, slot)
            else:
                forward(a, slot - 1, step).wait_recv()
            if send_on:
                copy = forward(a, slot, step)
                copy.start()
                forwards.append(copy)

    def valid(j):
        return jnp.where(z >= j, 1, 0) + jnp.where(z >= NZ - j, 1, 0)

    def peer(i):
        return jnp.where(i % 2 == 1, (i + 1) // 2, (8 - i // 2) % 8)

    def block_of(i):
        return (me8 + 8 - peer(i)) % 8

    def wait_query(i):
        @pl.when(i > 0)
        def _():
            for copy in q_copies(jnp.maximum(peer(i), 1)):
                copy.wait_recv()

    def own(i):
        wait_query(i)
        qb = block_of(i)

        @pl.when(qb // 2 >= y)
        def _():
            own_task(qb)

    for a in range(3):
        pltpu.make_async_copy(own_piece(a, c), kv_arrays[a][1].at[0, c], local_sem.at[a]).wait()
        remote(
            own_piece(a, 1 - c),
            kv_arrays[a][1].at[0, c],
            kv_send.at[a, 0, 0],
            kv_recv.at[a, 0, 0],
            partner,
            x,
        ).wait_recv()
    pltpu.make_async_copy(q_in.at[c], qbuf.at[me8], local_sem.at[3]).wait()
    pltpu.make_async_copy(f_in.at[c], fqbuf.at[me8], local_sem.at[4]).wait()
    make_bias(0)

    near = 4

    def stage_a(i, _):
        own(i)
        return 0

    lax.fori_loop(0, near, stage_a, 0)
    arrive(1, 1, True, True)
    arrive(5, -1, True, True)
    make_bias(1)
    make_bias(5)

    run_tasks(near * valid(1), lambda t: (1 + 4 * (t // near), block_of(t % near)))
    arrive(2, 1, False, True)
    arrive(6, -1, False, True)
    make_bias(2)
    make_bias(6)
    w_first[0].wait_recv()
    w_forward[0].start()
    w_first[1].wait_recv()
    w_forward[1].start()

    lax.fori_loop(near, 8, stage_a, 0)
    run_tasks(near * valid(1), lambda t: (1 + 4 * (t // near), block_of(near + t % near)))
    arrive(3, 1, False, True)
    arrive(7, -1, False, False)
    make_bias(3)
    make_bias(7)

    run_tasks(8 * valid(2), lambda t: (2 + 4 * (t // 8), block_of(t % 8)))
    arrive(4, 1, False, False)
    make_bias(4)
    w_first[2].wait_recv()
    w_partner[0].start()
    w_first[3].wait_recv()
    w_partner[1].start()

    def o_copy(r8, rx):
        to = (me8 + r8) % 8
        tx = (x + rx) % NX
        return (
            remote(
                obuf.at[to, pl.ds(tx * 64, 64)],
                rbuf.at[y, :, pl.ds((x * 2 + c) * 256, 256)],
                o_send.at[r8, rx],
                o_recv.at[r8, rx],
                zbase + to,
                tx,
            ),
            remote(
                lbuf.at[to, tx // 2],
                lrecv.at[y, x * 2 + c],
                l_send.at[r8, rx],
                l_recv.at[r8, rx],
                zbase + to,
                tx,
            ),
        )

    def finish(r):
        i = 7 - r
        qb = block_of(i)
        r8 = (8 - peer(i)) % 8
        sums = []
        for h in (0, 1):
            total = stats[qb, 2 + h : 3 + h, :]
            some = total > 0.0
            inv = jnp.where(some, 1.0 / jnp.where(some, total, 1.0), 0.0)
            obuf[qb, :, h * 128 : (h + 1) * 128] = (acc[qb, h] * inv).T.astype(jnp.bfloat16)
            sums.append(
                jnp.where(
                    some, stats[qb, h : h + 1, :] * scale + jnp.log2(jnp.where(some, total, 1.0)), NEG
                )
            )
        both = jnp.concatenate(sums + [jnp.zeros((6, 256), jnp.float32)], axis=0)
        lbuf[qb, 0] = both[:, :128]
        lbuf[qb, 1] = both[:, 128:]
        for rx in (2, 1, 3):
            for copy in o_copy(r8, rx):
                copy.start()

        @pl.when(r8 > 0)
        def _():
            for copy in o_copy(r8, 0):
                copy.start()

    last = jnp.where(z >= 3, 1, 0) + jnp.where(z >= 4, 1, 0) + jnp.where(z >= 5, 1, 0)
    per_block = jnp.maximum(last, 1)

    def last_place(t):
        k = t % per_block
        return jnp.where(k == 0, 3, jnp.where(k == 1, 4, 7)), block_of(7 - t // per_block)

    def leave(t):
        @pl.when(t % per_block == per_block - 1)
        def _():
            finish(t // per_block)

    run_tasks(8 * last, last_place, leave)

    def finish_early(r, _):
        finish(r)
        return 0

    lax.fori_loop(0, jnp.where(last == 0, 8, 0), finish_early, 0)
    w_forward[0].wait_recv()
    w_forward[1].wait_recv()
    w_partner[2].start()
    own_copies = (
        pltpu.make_async_copy(
            obuf.at[me8, pl.ds(x * 64, 64)],
            rbuf.at[y, :, pl.ds((x * 2 + c) * 256, 256)],
            local_sem.at[6],
        ),
        pltpu.make_async_copy(lbuf.at[me8, x // 2], lrecv.at[y, x * 2 + c], local_sem.at[7]),
    )
    for copy in own_copies:
        copy.start()
    for copy in own_copies:
        copy.wait()

    def wait_o(r, _):
        for copy in o_copy((r + 1) // NX, (r + 1) % NX):
            copy.wait_recv()
        return 0

    lax.fori_loop(0, 31, wait_o, 0)

    logs = [lrecv[i].reshape(64, 128) for i in range(NY)]
    top = jnp.maximum(jnp.maximum(logs[0], logs[1]), jnp.maximum(logs[2], logs[3]))
    parts = [jnp.exp2(v - top) for v in logs]
    inv = 1.0 / (parts[0] + parts[1] + parts[2] + parts[3])
    for i in range(NY):
        scaled = parts[i] * inv
        wcols[i] = jnp.concatenate([scaled, scaled], axis=0).T
    first_row = pl.multiple_of((x % 2) * 64, 64)
    shares = [wcols[i, pl.ds(first_row, 64), :] for i in range(NY)]
    for n in range(HEADS):
        lane = (n // 2) * 8 + n % 2
        cols = slice(n * 128, (n + 1) * 128)
        mixed = shares[0][:, lane : lane + 1] * rbuf[0, :, cols].astype(jnp.float32)
        for i in range(1, NY):
            mixed = mixed + shares[i][:, lane : lane + 1] * rbuf[i, :, cols].astype(jnp.float32)
        att[:, cols] = mixed.astype(jnp.bfloat16)

    pltpu.make_async_copy(w_in, wbuf.at[x], local_sem.at[5]).wait()
    pltpu.make_async_copy(res_in, res_ref, local_sem.at[8]).wait()
    pltpu.make_async_copy(gain_in, gain_ref, local_sem.at[9]).wait()
    for copy in w_partner:
        copy.wait_recv()

    width = w_in.shape[1]
    chunk = 256

    def project(i, total):
        cols = pl.ds(pl.multiple_of(i * chunk, chunk), chunk)
        part = jnp.dot(att[:, 0:512], wbuf[0, :, cols], preferred_element_type=jnp.float32)
        for b in range(1, NX):
            part = part + jnp.dot(
                att[:, b * 512 : (b + 1) * 512],
                wbuf[b, :, cols],
                preferred_element_type=jnp.float32,
            )
        stream = (res_ref[:, cols].astype(jnp.float32) + part).astype(jnp.bfloat16)
        stream_ref[:, cols] = stream
        wide = stream.astype(jnp.float32)
        return total + jnp.sum(wide * wide, axis=1, keepdims=True)

    total = lax.fori_loop(0, width // chunk, project, jnp.zeros((64, 1), jnp.float32))
    rate = lax.rsqrt(total * (1.0 / width) + norm_eps)
    normed_ref[...] = (stream_ref[...].astype(jnp.float32) * rate * gain_ref[...]).astype(
        jnp.bfloat16
    )

    for copy in first_sends + forwards + w_first + w_forward + w_partner:
        copy.wait_send()

    def wait_q(i, _):
        for copy in q_copies(i + 1):
            copy.wait_send()
        return 0

    lax.fori_loop(0, 7, wait_q, 0)

    def wait_sent(r, _):
        for copy in o_copy((r + 1) // NX, (r + 1) % NX):
            copy.wait_send()
        return 0

    lax.fori_loop(0, 31, wait_sent, 0)


def attention(residual, queries, key_rows, value_rows, forget_sums, out_weight, norm_gain):
    rows, width = residual.shape
    tokens = queries.shape[0]
    q_in = queries.T.reshape(2, 256, tokens)
    v_in = value_rows.T.reshape(2, 128, tokens)
    bf16, f32 = jnp.bfloat16, jnp.float32
    anywhere = pl.BlockSpec(memory_space=pl.ANY)
    hbm = pl.BlockSpec(memory_space=pl.ANY)
    vmem = pl.BlockSpec(memory_space=pltpu.VMEM)
    dma = pltpu.SemaphoreType.DMA
    return pl.pallas_call(
        attention_kernel,
        out_shape=(
            jax.ShapeDtypeStruct((rows, width), bf16),
            jax.ShapeDtypeStruct((rows, width), bf16),
        ),
        in_specs=[anywhere, hbm, anywhere, vmem, hbm, hbm, hbm],
        out_specs=(vmem, vmem),
        scratch_shapes=[
            pltpu.VMEM((8, 256, 256), bf16),
            pltpu.VMEM((8, 8, 256), f32),
            pltpu.VMEM((8, 2, 256, 128), bf16),
            pltpu.VMEM((8, 2, 128, 256), bf16),
            pltpu.VMEM((8, 2, 8, 256), f32),
            pltpu.VMEM((2, 8, 256), f32),
            pltpu.VMEM((8, 2, 256, 128), bf16),
            pltpu.VMEM((2, 128, 256), bf16),
            pltpu.VMEM((2, 2, 256, 256), f32),
            pltpu.VMEM((2, 2, 256, 256), f32),
            pltpu.VMEM((64, 2048), bf16),
            pltpu.VMEM((1, 2048), f32),
            pltpu.VMEM((8, 2, 128, 256), f32),
            pltpu.VMEM((8, 8, 256), f32),
            pltpu.VMEM((8, 256, 256), bf16),
            pltpu.VMEM((8, 2, 8, 128), f32),
            pltpu.VMEM((4, 64, 2048), bf16),
            pltpu.VMEM((4, 8, 8, 128), f32),
            pltpu.VMEM((4, 128, 128), f32),
            pltpu.VMEM((64, 2048), bf16),
            pltpu.VMEM((4, 512, 2048), bf16),
            dma((2, 8)),
            dma((2, 8)),
            dma((3, 8, 2)),
            dma((3, 8, 2)),
            dma((8, 4)),
            dma((8, 4)),
            dma((8, 4)),
            dma((8, 4)),
            dma((6,)),
            dma((6,)),
            dma((3,)),
            dma((3,)),
            dma((10,)),
        ],
        compiler_params=pltpu.CompilerParams(
            collective_id=0, has_side_effects=True, vmem_limit_bytes=66_000_000
        ),
        cost_estimate=pl.CostEstimate(
            flops=8 * 10**9, bytes_accessed=16 * 2**20, transcendentals=16 * 2**20
        ),
    )(q_in, key_rows, v_in, forget_sums.T, out_weight, residual, norm_gain.reshape(1, width))


def experts_kernel(
    normed_ref,
    stream_ref,
    ids_ref,
    route_ref,
    eg_in,
    eu_in,
    ed_in,
    sg_in,
    su_in,
    sd_in,
    out_ref,
    nbuf,
    table,
    tables,
    sel,
    gate,
    sbuf,
    xbuf,
    obuf,
    rbuf,
    cin,
    cout,
    total,
    eg,
    eu,
    ed,
    sg,
    su,
    sd,
    n_send,
    n_recv,
    t_send,
    t_recv,
    x_send,
    x_recv,
    r_send,
    r_recv,
    c_send,
    c_recv,
    w_sem,
    x_sem,
    r_sem,
):
    sp = lax.axis_index("sp")
    x = lax.axis_index("tp")
    z = sp // 8
    me8 = sp % 8
    zbase = z * 8
    width = normed_ref.shape[1]
    half = width // 2

    def at_z(step):
        return ((z + step + NZ) % NZ) * 8 + me8

    barrier = pltpu.get_barrier_semaphore()
    for r in range(1, 8):
        for to in (zbase + (me8 + r) % 8, at_z(r)):
            pl.semaphore_signal(barrier, inc=1, device_id=(to, x), device_id_type=MESH)
    loads = [
        pltpu.make_async_copy(src, dst, w_sem.at[i])
        for i, (src, dst) in enumerate(
            (
                (sg_in, sg),
                (su_in, su),
                (sd_in, sd),
                (eg_in.at[0], eg),
                (eu_in.at[0], eu),
                (ed_in.at[0], ed),
            )
        )
    ]
    for copy in loads:
        copy.start()
    nbuf[0, 0] = normed_ref[:, :half]
    nbuf[0, 1] = normed_ref[:, half:]
    pl.semaphore_wait(barrier, 14)

    def remote(src, dst, send, recv, sp_id):
        return pltpu.make_async_remote_copy(
            src_ref=src,
            dst_ref=dst,
            send_sem=send,
            recv_sem=recv,
            device_id=(sp_id, x),
            device_id_type=MESH,
        )

    def pass_on(slot, to_slot, hf, step):
        return remote(
            nbuf.at[slot, hf],
            nbuf.at[to_slot, hf],
            n_send.at[to_slot, hf],
            n_recv.at[to_slot, hf],
            at_z(step),
        )

    sent = []

    def send(copy):
        copy.start()
        sent.append(copy)

    up, down = 1, 1 + UP_STEPS
    for hf in (0, 1):
        send(pass_on(0, up, hf, 1))
        send(pass_on(0, down, hf, -1))

    f32, bf16 = jnp.float32, jnp.bfloat16
    ids = ids_ref[...]
    weights = route_ref[...]
    gates = weights / jnp.sum(weights, axis=1, keepdims=True) * routed_scale
    rows = ids.shape[0]
    experts = lax.broadcasted_iota(jnp.int32, (rows, 64), 1)
    named = jnp.zeros((rows, 64), f32)
    shares = jnp.zeros((rows, 64), f32)
    for k in range(TOPK):
        hit = ids[:, k : k + 1] == experts
        named = named + jnp.where(hit, 1.0, 0.0)
        shares = shares + jnp.where(hit, gates[:, k : k + 1], 0.0)
    earlier = (
        lax.broadcasted_iota(jnp.int32, (rows, rows), 1)
        < lax.broadcasted_iota(jnp.int32, (rows, rows), 0)
    )
    named = named.astype(bf16)
    rank = jnp.dot(jnp.where(earlier, 1.0, 0.0).astype(bf16), named, preferred_element_type=f32)
    lane = lax.broadcasted_iota(jnp.int32, (64, 1024), 1)
    expert = lax.broadcasted_iota(jnp.int32, (64, 1024), 0)
    spread = jnp.where(lane // 16 == expert, 1.0, 0.0).astype(bf16)
    named_x = jnp.dot(named, spread, preferred_element_type=f32)
    rank_x = jnp.dot(rank.astype(bf16), spread, preferred_element_type=f32)
    share_x = jnp.dot(shares.astype(bf16), spread, preferred_element_type=f32)
    want = (lax.broadcasted_iota(jnp.int32, (rows, 1024), 1) % 8).astype(f32)
    filled = jnp.where(rank_x == want, named_x, 0.0)
    token = lax.broadcasted_iota(jnp.int32, (rows, 1024), 0).astype(f32)
    source = jnp.sum(filled * (token + 1000.0), axis=0, keepdims=True) - 1000.0
    share = jnp.sum(filled * share_x, axis=0, keepdims=True)
    for p in range(NZ):
        lanes = slice(p * 128, (p + 1) * 128)
        table[p] = jnp.concatenate(
            [source[:, lanes], share[:, lanes], jnp.zeros((6, 128), f32)], axis=0
        )
    tables[z] = table[z]

    def table_copy(r):
        to = (z + r) % NZ
        return remote(table.at[to], tables.at[z], t_send.at[r], t_recv.at[r], to * 8 + me8)

    for r in range(1, NZ):
        send(table_copy(r))

    for copy in loads[:3]:
        copy.wait()
    n = normed_ref[...]
    g = jnp.dot(n, sg[...], preferred_element_type=f32)
    u = jnp.dot(n, su[...], preferred_element_type=f32)
    hidden = (g / (1.0 + jnp.exp(-g)) * u).astype(bf16)
    for i in range(4):
        cols = slice(i * width // 4, (i + 1) * width // 4)
        total[:, cols] = stream_ref[:, cols].astype(f32) + jnp.dot(
            hidden, sd[:, cols], preferred_element_type=f32
        )

    pairs = ((1, 5), (2, 6), (3, 7), (4, 0))
    offset = {0: 0, 1: -1, 2: -2, 3: -3, 4: -4, 5: 1, 6: 2, 7: 3}

    def arrive(slot, step, send_on):
        for hf in (0, 1):
            pass_on(slot - 1 if slot not in (up, down) else 0, slot, hf, step).wait_recv()
            if send_on:
                send(pass_on(slot, slot + 1, hf, step))

    def x_copy(b, r):
        to = (me8 + r) % 8
        return remote(sbuf.at[b, to], xbuf.at[b, me8], x_send.at[b, r], x_recv.at[b, r], zbase + to)

    def r_copy(b, r):
        to = (me8 + r) % 8
        return remote(obuf.at[b, to], rbuf.at[b, me8], r_send.at[b, r], r_recv.at[b, r], zbase + to)

    def x_own(b):
        return pltpu.make_async_copy(sbuf.at[b, me8], xbuf.at[b, me8], x_sem.at[b])

    def r_own(b):
        return pltpu.make_async_copy(obuf.at[b, me8], rbuf.at[b, me8], r_sem.at[b])

    def dispatch(b):
        first, second = pairs[b]
        ta = tables[(z + offset[first] + NZ) % NZ]
        tb = tables[(z + offset[second] + NZ) % NZ]
        lane_of = lax.broadcasted_iota(jnp.int32, (1, 128), 1) % 16
        src = jnp.where(lane_of < 8, ta[0:1], tb[0:1] + 64.0)
        share_row = jnp.where(lane_of < 8, ta[1:2], tb[1:2])
        token_of = lax.broadcasted_iota(jnp.int32, (128, 128), 0).astype(f32)
        chosen = jnp.where(token_of == src, 1.0, 0.0)
        sel[...] = chosen.T.astype(bf16)
        gate[b] = (chosen * share_row).astype(bf16)
        for hf in (0, 1):
            for i in range(2):
                cols = slice(i * half // 2, (i + 1) * half // 2)
                tokens = jnp.concatenate([nbuf[first, hf, :, cols], nbuf[second, hf, :, cols]], axis=0)
                picked = jnp.dot(sel[...], tokens, preferred_element_type=f32)
                at = hf * half + i * half // 2
                sbuf[b, :, :, at : at + half // 2] = picked.astype(bf16).reshape(8, 16, half // 2)
        for r in (4, 3, 5, 2, 6, 1, 7):
            send(x_copy(b, r))
        x_own(b).start()

    def run_expert(b):
        for r in range(1, 8):
            x_copy(b, r).wait_recv()
        x_own(b).wait()
        rows_in = xbuf[b].reshape(128, width)
        g = jnp.dot(rows_in, eg[...], preferred_element_type=f32)
        u = jnp.dot(rows_in, eu[...], preferred_element_type=f32)
        hidden = (g / (1.0 + jnp.exp(-g)) * u).astype(bf16)
        for i in range(4):
            cols = slice(i * width // 4, (i + 1) * width // 4)
            made = jnp.dot(hidden, ed[:, cols], preferred_element_type=f32)
            obuf[b, :, :, cols] = made.astype(bf16).reshape(8, 16, width // 4)

    def give_back(b):
        for r in (4, 3, 5, 2, 6, 1, 7):
            send(r_copy(b, r))
        r_own(b).start()

    def need_tables(*steps):
        for r in steps:
            table_copy(r).wait_recv()

    arrive(1, 1, True)
    arrive(5, -1, True)
    need_tables(1, 7)
    dispatch(0)
    for copy in loads[3:]:
        copy.wait()
    arrive(2, 1, True)
    arrive(6, -1, True)
    need_tables(2, 6)
    dispatch(1)
    run_expert(0)
    arrive(3, 1, True)
    arrive(7, -1, False)
    need_tables(3, 5)
    dispatch(2)
    run_expert(1)
    arrive(4, 1, False)
    need_tables(4)
    dispatch(3)
    run_expert(2)
    run_expert(3)
    give_back(3)
    give_back(2)
    give_back(1)
    give_back(0)

    def chain_copy(way, place, hf):
        return remote(
            cout.at[way, place, hf],
            cin.at[way, place, hf],
            c_send.at[way, place, hf],
            c_recv.at[way, place, hf],
            at_z(-1 if way == 0 else 1),
        )

    for b, places in ((3, (3, None)), (2, (2, 2)), (1, (1, 1)), (0, (0, 0))):
        for r in range(1, 8):
            r_copy(b, r).wait_recv()
        r_own(b).wait()
        for hf in (0, 1):
            cols = slice(hf * half, (hf + 1) * half)
            part = jnp.dot(
                gate[b], rbuf[b, :, :, cols].reshape(128, half), preferred_element_type=f32
            )
            for way in (0, 1):
                mine = part[way * 64 : (way + 1) * 64]
                place = places[way]
                if place is None:
                    total[:, cols] = total[:, cols] + mine
                    continue
                if place < (3 if way == 0 else 2):
                    chain_copy(way, place + 1, hf).wait_recv()
                    mine = mine + cin[way, place + 1, hf].astype(f32)
                cout[way, place, hf] = mine.astype(bf16)
                send(chain_copy(way, place, hf))
    for hf in (0, 1):
        cols = slice(hf * half, (hf + 1) * half)
        for way in (0, 1):
            chain_copy(way, 0, hf).wait_recv()
        out_ref[:, cols] = (
            total[:, cols] + cin[0, 0, hf].astype(f32) + cin[1, 0, hf].astype(f32)
        ).astype(bf16)
    for copy in sent:
        copy.wait_send()


def experts(
    normed,
    stream,
    expert_ids,
    route_weights,
    expert_gate,
    expert_up,
    expert_down,
    shared_gate,
    shared_up,
    shared_down,
):
    rows, width = normed.shape
    hidden = expert_gate.shape[2]
    shared = shared_gate.shape[1]
    bf16, f32 = jnp.bfloat16, jnp.float32
    hbm = pl.BlockSpec(memory_space=pl.ANY)
    vmem = pl.BlockSpec(memory_space=pltpu.VMEM)
    dma = pltpu.SemaphoreType.DMA
    return pl.pallas_call(
        experts_kernel,
        out_shape=jax.ShapeDtypeStruct((rows, width), bf16),
        in_specs=[vmem] * 4 + [hbm] * 6,
        out_specs=vmem,
        scratch_shapes=[
            pltpu.VMEM((8, 2, rows, width // 2), bf16),
            pltpu.VMEM((8, 8, 128), f32),
            pltpu.VMEM((8, 8, 128), f32),
            pltpu.VMEM((128, 128), bf16),
            pltpu.VMEM((4, 128, 128), bf16),
            pltpu.VMEM((4, 8, 16, width), bf16),
            pltpu.VMEM((4, 8, 16, width), bf16),
            pltpu.VMEM((4, 8, 16, width), bf16),
            pltpu.VMEM((4, 8, 16, width), bf16),
            pltpu.VMEM((2, 4, 2, rows, width // 2), bf16),
            pltpu.VMEM((2, 4, 2, rows, width // 2), bf16),
            pltpu.VMEM((rows, width), f32),
            pltpu.VMEM((width, hidden), bf16),
            pltpu.VMEM((width, hidden), bf16),
            pltpu.VMEM((hidden, width), bf16),
            pltpu.VMEM((width, shared), bf16),
            pltpu.VMEM((width, shared), bf16),
            pltpu.VMEM((shared, width), bf16),
            dma((8, 2)),
            dma((8, 2)),
            dma((8,)),
            dma((8,)),
            dma((4, 8)),
            dma((4, 8)),
            dma((4, 8)),
            dma((4, 8)),
            dma((2, 4, 2)),
            dma((2, 4, 2)),
            dma((6,)),
            dma((4,)),
            dma((4,)),
        ],
        compiler_params=pltpu.CompilerParams(
            collective_id=1, has_side_effects=True, vmem_limit_bytes=66_000_000
        ),
        cost_estimate=pl.CostEstimate(
            flops=4 * 10**9, bytes_accessed=16 * 2**20, transcendentals=2**20
        ),
    )(
        normed,
        stream,
        expert_ids,
        route_weights,
        expert_gate,
        expert_up,
        expert_down,
        shared_gate,
        shared_up,
        shared_down,
    )


def local(
    residual,
    queries,
    key_rows,
    value_rows,
    forget_sums,
    out_weight,
    norm_gain,
    expert_ids,
    route_weights,
    expert_gate,
    expert_up,
    expert_down,
    shared_gate,
    shared_up,
    shared_down,
):
    stream, normed = attention(
        residual, queries, key_rows, value_rows, forget_sums, out_weight, norm_gain
    )
    return experts(
        normed,
        stream,
        expert_ids,
        route_weights,
        expert_gate,
        expert_up,
        expert_down,
        shared_gate,
        shared_up,
        shared_down,
    )


def solution(mesh):
    in_specs = (
        P(("sp", "tp"), None),
        P("sp", "tp"),
        P("sp", "tp"),
        P("sp", "tp"),
        P("sp", "tp"),
        P("tp", None),
        P(),
        P(("sp", "tp"), None),
        P(("sp", "tp"), None),
        P("sp", None, None),
        P("sp", None, None),
        P("sp", None, None),
        P(),
        P(),
        P(),
    )
    out_specs = P(("sp", "tp"), None)
    return jax.shard_map(local, mesh=mesh, in_specs=in_specs, out_specs=out_specs, check_vma=False)
```

```python
import jax
import jax.numpy as jnp
from jax import lax
from jax.experimental import pallas as pl
from jax.experimental.pallas import tpu as pltpu
from jax.sharding import PartitionSpec as P

HEADS = 16
KV_HEADS = 8
HEAD_DIM = 128
TOPK = 4
MESH = pl.DeviceIdType.MESH
LOG2E = 1.4426950408889634
NEG = -1e30

routed_scale = 2.5
norm_eps = 1e-06

NZ, NY, NX = 8, 4, 4
UP_STEPS, DOWN_STEPS = 4, 3


def attention_kernel(
    prepare,
    q_in,
    k_rows,
    v_in,
    f_rows,
    w_in,
    res_in,
    gain_in,
    stream_ref,
    normed_ref,
    qbuf,
    fqbuf,
    kbuf,
    vbuf,
    fbuf,
    f_in,
    bias,
    ones,
    held_a,
    held_b,
    res_ref,
    gain_ref,
    acc,
    stats,
    obuf,
    lbuf,
    rbuf,
    lrecv,
    wcols,
    att,
    wbuf,
    q_send,
    q_recv,
    kv_send,
    kv_recv,
    o_send,
    o_recv,
    l_send,
    l_recv,
    w_send,
    w_recv,
    s_send,
    s_recv,
    p_send,
    p_recv,
    local_sem,
):
    sp = lax.axis_index("sp")
    x = lax.axis_index("tp")
    z = sp // 8
    me8 = sp % 8
    y = me8 // 2
    c = me8 % 2
    zbase = z * 8

    def at_z(step, core):
        return ((z + step + NZ) % NZ) * 8 + y * 2 + core

    partner = zbase + y * 2 + (1 - c)
    xr = (x + 1) % NX
    xl = (x + NX - 1) % NX

    barrier = pltpu.get_barrier_semaphore()

    def greet_plane(i, _):
        n = i + 1
        r8, rx = n // NX, n % NX
        pl.semaphore_signal(
            barrier,
            inc=1,
            device_id=(zbase + (me8 + r8) % 8, (x + rx) % NX),
            device_id_type=MESH,
        )
        return 0

    lax.fori_loop(0, 31, greet_plane, 0)
    for step in range(2, NZ - 1):
        pl.semaphore_signal(barrier, inc=1, device_id=(at_z(step, c), x), device_id_type=MESH)
    for step in (1, -1):
        for core in (0, 1):
            pl.semaphore_signal(
                barrier, inc=1, device_id=(at_z(step, core), x), device_id_type=MESH
            )
    pltpu.make_async_copy(q_in.at[c], qbuf.at[me8], local_sem.at[3]).start()
    pltpu.make_async_copy(w_in, wbuf.at[x], local_sem.at[5]).start()
    pltpu.make_async_copy(res_in, res_ref, local_sem.at[8]).start()
    pltpu.make_async_copy(gain_in, gain_ref, local_sem.at[9]).start()
    for h in (0, 1):
        f_in[h] = jnp.concatenate(
            [f_rows[2 * h : 2 * h + 2, :], jnp.zeros((6, f_rows.shape[1]), jnp.float32)], axis=0
        )
        row = lax.broadcasted_iota(jnp.int32, (128, 256), 0)
        ones[h] = jnp.where((row % 8 == h) & (row < 24), 1.0, 0.0).astype(jnp.bfloat16)
    acc[...] = jnp.zeros_like(acc)
    row = lax.broadcasted_iota(jnp.int32, stats.shape, 1)
    stats[...] = jnp.where(row < 2, NEG, 0.0)
    pl.semaphore_wait(barrier, 40)

    def remote(src, dst, send, recv, sp_id, tp_id):
        return pltpu.make_async_remote_copy(
            src_ref=src,
            dst_ref=dst,
            send_sem=send,
            recv_sem=recv,
            device_id=(sp_id, tp_id),
            device_id_type=MESH,
        )

    kv_arrays = ((k_rows, kbuf), (v_in, vbuf), (f_in, fbuf))

    def own_piece(a, h):
        if a == 0:
            return k_rows.at[:, pl.ds(pl.multiple_of(h * 128, 128), 128)]
        return kv_arrays[a][0].at[h]

    first_sends = []
    for a in (2, 0, 1):
        dst = kv_arrays[a][1]
        pltpu.make_async_copy(own_piece(a, c), dst.at[0, c], local_sem.at[a]).start()
        first_sends.append(
            remote(
                own_piece(a, 1 - c),
                dst.at[0, c],
                kv_send.at[a, 0, 0],
                kv_recv.at[a, 0, 0],
                partner,
                x,
            )
        )
        for step, slot in ((1, 1), (-1, 1 + UP_STEPS)):
            for h in (0, 1):
                first_sends.append(
                    remote(
                        own_piece(a, h),
                        dst.at[slot, c],
                        kv_send.at[a, slot, h],
                        kv_recv.at[a, slot, c],
                        at_z(step, h),
                        x,
                    )
                )
    for copy in first_sends:
        copy.start()

    pltpu.make_async_copy(f_in.at[c], fqbuf.at[me8], local_sem.at[4]).start()

    def q_copies(r):
        to = (me8 + r) % 8
        return (
            remote(f_in.at[to % 2], fqbuf.at[me8], q_send.at[1, r], q_recv.at[1, r], zbase + to, x),
            remote(q_in.at[to % 2], qbuf.at[me8], q_send.at[0, r], q_recv.at[0, r], zbase + to, x),
        )

    def start_q(i, _):
        for copy in q_copies(i + 1):
            copy.start()
        return 0

    lax.fori_loop(0, 7, start_q, 0)

    mine = w_in.shape[0] // 2
    shared_rows = mine // 4
    part = shared_rows // NY
    direct = mine - shared_rows
    eighth = direct // 2
    top_row = c * mine
    rows_a = pl.ds(top_row, direct)
    rows_a0 = pl.ds(top_row, eighth)
    rows_a1 = pl.ds(top_row + eighth, eighth)
    rows_b = pl.ds(top_row + direct, shared_rows)
    across = (x + 2) % NX
    others = (xl, xr, across)

    def share_rows(yy):
        return pl.ds(top_row + direct + yy * part, part)

    def x_of(i, step):
        return (x + step * (1, -1, 2)[i] + NX) % NX

    w_share = [
        remote(
            w_in.at[share_rows(y)], wbuf.at[x, share_rows(y)], w_send.at[i], w_recv.at[i], sp, x_of(i, 1)
        )
        for i in range(3)
    ]
    w_first = [
        remote(w_in.at[rows_a0], wbuf.at[x, rows_a0], w_send.at[3], w_recv.at[3], sp, xr),
        remote(w_in.at[rows_a1], wbuf.at[x, rows_a1], w_send.at[4], w_recv.at[4], sp, xl),
        remote(w_in.at[rows_a1], wbuf.at[x, rows_a1], w_send.at[5], w_recv.at[5], sp, xr),
        remote(w_in.at[rows_a0], wbuf.at[x, rows_a0], w_send.at[6], w_recv.at[6], sp, xl),
    ]
    for copy in w_share + w_first:
        copy.start()
    w_forward = [
        remote(wbuf.at[xl, rows_a0], wbuf.at[xl, rows_a0], w_send.at[7], w_recv.at[7], sp, xr),
        remote(wbuf.at[xr, rows_a1], wbuf.at[xr, rows_a1], w_send.at[8], w_recv.at[8], sp, xl),
    ]
    w_spread = [
        [
            remote(
                wbuf.at[o, share_rows(y)],
                wbuf.at[o, share_rows(y)],
                s_send.at[i, dy],
                s_recv.at[i, dy],
                zbase + ((y + dy) % NY) * 2 + c,
                x,
            )
            for dy in range(1, NY)
        ]
        for i, o in enumerate(others)
    ]
    w_partner = [
        [
            remote(wbuf.at[o, rows], wbuf.at[o, rows], p_send.at[i, k], p_recv.at[i, k], partner, x)
            for k, rows in enumerate((rows_a, rows_b))
        ]
        for i, o in enumerate(others)
    ]
    partner_copies = [copy for row in w_partner for copy in row]
    spread_copies = [copy for row in w_spread for copy in row]

    prepare()

    scale = HEAD_DIM ** (-0.5) * LOG2E
    root = HEAD_DIM**0.5

    def make_bias(slot):
        f0 = fbuf[slot, 0]
        base = f0[:, 0:1]
        for cc in (0, 1):
            rest = (base - (f0 if cc == 0 else fbuf[slot, 1])) * root
            pieces = []
            for _ in range(3):
                piece = rest.astype(jnp.bfloat16).astype(jnp.float32)
                pieces.append(piece)
                rest = rest - piece
            pieces.append(jnp.zeros((104, 256), jnp.float32))
            bias[slot, cc] = jnp.concatenate(pieces, axis=0).T.astype(jnp.bfloat16)

    def score(slot, qb, h, cc):
        q_h = jnp.concatenate([qbuf[qb, h * 128 : (h + 1) * 128, :], ones[h]], axis=0)
        keys = jnp.concatenate([kbuf[slot, cc], bias[slot, cc]], axis=1)
        return jnp.dot(keys, q_h, preferred_element_type=jnp.float32)

    span = 64

    def weigh(slot, qb, h, held):
        delta = (fqbuf[qb, h : h + 1, 0:1] - fbuf[slot, 0, h : h + 1, 0:1]) * root
        pieces = [(cc, slice(r, r + span)) for cc in (0, 1) for r in range(0, 256, span)]
        top = None
        for cc, part in pieces:
            high = jnp.max(held[h, cc, part, :].reshape(span // 8, 8, 256), axis=0)
            top = high if top is None else jnp.maximum(top, high)
        top = jnp.max(top, axis=0, keepdims=True)
        old = stats[qb, h : h + 1, :]
        new = jnp.maximum(old, top + delta)
        shift = new - delta
        factor = jnp.exp2((old - new) * scale)
        total = jnp.zeros((8, 256), jnp.float32)
        p = ([], [])
        for cc, part in pieces:
            e = jnp.exp2((held[h, cc, part, :] - shift) * scale)
            total = total + jnp.sum(e.reshape(span // 8, 8, 256), axis=0)
            p[cc].append(e.astype(jnp.bfloat16))
        total = jnp.sum(total, axis=0, keepdims=True)
        stats[qb, h : h + 1, :] = new
        stats[qb, 2 + h : 3 + h, :] = stats[qb, 2 + h : 3 + h, :] * factor + total
        mixed = jnp.dot(
            vbuf[slot, 0], jnp.concatenate(p[0], axis=0), preferred_element_type=jnp.float32
        ) + jnp.dot(vbuf[slot, 1], jnp.concatenate(p[1], axis=0), preferred_element_type=jnp.float32)
        acc[qb, h] = acc[qb, h] * factor + mixed

    def own_task(qb):
        rows = lax.broadcasted_iota(jnp.int32, (256, 256), 0)
        cols = lax.broadcasted_iota(jnp.int32, (256, 256), 1)
        gap = (qb - 2 * y) * 256
        for h in (0, 1):
            for cc in (0, 1):
                held_a[h, cc] = jnp.where(
                    rows + cc * 256 <= cols + gap, score(0, qb, h, cc), -jnp.inf
                )
        use(held_a, 0, qb)

    def fill(held, slot, qb):
        for h in (0, 1):
            for cc in (0, 1):
                held[h, cc] = score(slot, qb, h, cc)

    def use(held, slot, qb):
        for h in (0, 1):
            weigh(slot, qb, h, held)

    def run_tasks(count, place, after=None):
        @pl.when(count > 0)
        def _():
            fill(held_a, *place(0))

        def pair(i, _):
            first, second = 2 * i, 2 * i + 1
            fill(held_b, *place(second))
            use(held_a, *place(first))
            if after is not None:
                after(first)
            fill(held_a, *place(jnp.minimum(second + 1, count - 1)))
            use(held_b, *place(second))
            if after is not None:
                after(second)
            return 0

        lax.fori_loop(0, count // 2, pair, 0)

    def wait_first(a, slot):
        for h in (0, 1):
            remote(
                own_piece(a, h),
                kv_arrays[a][1].at[slot, h],
                kv_send.at[a, slot, h],
                kv_recv.at[a, slot, h],
                partner,
                x,
            ).wait_recv()

    def forward(a, slot, step):
        buf = kv_arrays[a][1]
        if slot in (UP_STEPS - 1, UP_STEPS + DOWN_STEPS):
            piece = 0 if slot == UP_STEPS - 1 else 1
            return remote(
                buf.at[slot, piece],
                buf.at[UP_STEPS, piece],
                kv_send.at[a, UP_STEPS, piece],
                kv_recv.at[a, UP_STEPS, piece],
                at_z(step, c),
                x,
            )
        return remote(
            buf.at[slot],
            buf.at[slot + 1],
            kv_send.at[a, slot + 1, 0],
            kv_recv.at[a, slot + 1, 0],
            at_z(step, c),
            x,
        )

    forwards = []

    def arrive(slot, step, first, send_on):
        for a in (2, 0, 1):
            if first:
                wait_first(a, slot)
            else:
                forward(a, slot - 1, step).wait_recv()
            if send_on:
                copy = forward(a, slot, step)
                copy.start()
                forwards.append(copy)

    def valid(j):
        return jnp.where(z >= j, 1, 0) + jnp.where(z >= NZ - j, 1, 0)

    def peer(i):
        return jnp.where(i % 2 == 1, (i + 1) // 2, (8 - i // 2) % 8)

    def block_of(i):
        return (me8 + 8 - peer(i)) % 8

    def wait_query(i):
        @pl.when(i > 0)
        def _():
            for copy in q_copies(jnp.maximum(peer(i), 1)):
                copy.wait_recv()

    def own(i):
        wait_query(i)
        qb = block_of(i)

        @pl.when(qb // 2 >= y)
        def _():
            own_task(qb)

    for a in range(3):
        pltpu.make_async_copy(own_piece(a, c), kv_arrays[a][1].at[0, c], local_sem.at[a]).wait()
        remote(
            own_piece(a, 1 - c),
            kv_arrays[a][1].at[0, c],
            kv_send.at[a, 0, 0],
            kv_recv.at[a, 0, 0],
            partner,
            x,
        ).wait_recv()
    pltpu.make_async_copy(q_in.at[c], qbuf.at[me8], local_sem.at[3]).wait()
    pltpu.make_async_copy(f_in.at[c], fqbuf.at[me8], local_sem.at[4]).wait()
    make_bias(0)

    near = 4

    def stage_a(i, _):
        own(i)
        return 0

    lax.fori_loop(0, near, stage_a, 0)
    arrive(1, 1, True, True)
    arrive(5, -1, True, True)
    for i in range(3):
        w_share[i].wait_recv()
        for copy in w_spread[i]:
            copy.start()
    make_bias(1)
    make_bias(5)

    run_tasks(near * valid(1), lambda t: (1 + 4 * (t // near), block_of(t % near)))
    arrive(2, 1, False, True)
    arrive(6, -1, False, True)
    make_bias(2)
    make_bias(6)
    w_first[0].wait_recv()
    w_forward[0].start()
    w_first[1].wait_recv()
    w_forward[1].start()

    lax.fori_loop(near, 8, stage_a, 0)
    run_tasks(near * valid(1), lambda t: (1 + 4 * (t // near), block_of(near + t % near)))
    arrive(3, 1, False, True)
    arrive(7, -1, False, True)
    make_bias(3)
    make_bias(7)
    run_tasks(8 * valid(2), lambda t: (2 + 4 * (t // 8), block_of(t % 8)))
    w_first[2].wait_recv()
    w_first[3].wait_recv()
    w_partner[0][0].start()
    w_partner[1][0].start()
    run_tasks(8 * valid(3), lambda t: (3 + 4 * (t // 8), block_of(t % 8)))
    w_forward[0].wait_recv()
    w_forward[1].wait_recv()
    w_partner[2][0].start()
    for a in (2, 0, 1):
        forward(a, 3, 1).wait_recv()
        forward(a, 7, -1).wait_recv()
    make_bias(4)

    def o_copy(r8, rx):
        to = (me8 + r8) % 8
        tx = (x + rx) % NX
        return (
            remote(
                obuf.at[to, pl.ds(tx * 64, 64)],
                rbuf.at[y, x * 2 + c],
                o_send.at[r8, rx],
                o_recv.at[r8, rx],
                zbase + to,
                tx,
            ),
            remote(
                lbuf.at[to, tx // 2],
                lrecv.at[y, x * 2 + c],
                l_send.at[r8, rx],
                l_recv.at[r8, rx],
                zbase + to,
                tx,
            ),
        )

    def finish(r):
        i = 7 - r
        qb = block_of(i)
        r8 = (8 - peer(i)) % 8
        sums = []
        for h in (0, 1):
            total = stats[qb, 2 + h : 3 + h, :]
            some = total > 0.0
            inv = jnp.where(some, 1.0 / jnp.where(some, total, 1.0), 0.0)
            obuf[qb, :, h * 128 : (h + 1) * 128] = (acc[qb, h] * inv).T.astype(jnp.bfloat16)
            sums.append(
                jnp.where(
                    some, stats[qb, h : h + 1, :] * scale + jnp.log2(jnp.where(some, total, 1.0)), NEG
                )
            )
        both = jnp.concatenate(sums + [jnp.zeros((6, 256), jnp.float32)], axis=0)
        lbuf[qb, 0] = both[:, :128]
        lbuf[qb, 1] = both[:, 128:]
        for rx in (2, 1, 3):
            for copy in o_copy(r8, rx):
                copy.start()

        @pl.when(r8 > 0)
        def _():
            for copy in o_copy(r8, 0):
                copy.start()

    last = jnp.where(z >= UP_STEPS, 1, 0)

    def last_place(t):
        return UP_STEPS, block_of(7 - t)

    def leave(t):
        finish(t)

    run_tasks(8 * last, last_place, leave)

    def finish_early(r, _):
        finish(r)
        return 0

    lax.fori_loop(0, jnp.where(last == 0, 8, 0), finish_early, 0)
    for copy in spread_copies:
        copy.wait_recv()
    for row in w_partner:
        row[1].start()
    own_copies = (
        pltpu.make_async_copy(
            obuf.at[me8, pl.ds(x * 64, 64)],
            rbuf.at[y, x * 2 + c],
            local_sem.at[6],
        ),
        pltpu.make_async_copy(lbuf.at[me8, x // 2], lrecv.at[y, x * 2 + c], local_sem.at[7]),
    )
    for copy in own_copies:
        copy.start()
    for copy in own_copies:
        copy.wait()

    def wait_o(r, _):
        for copy in o_copy((r + 1) // NX, (r + 1) % NX):
            copy.wait_recv()
        return 0

    lax.fori_loop(0, 31, wait_o, 0)

    logs = [lrecv[i].reshape(64, 128) for i in range(NY)]
    top = jnp.maximum(jnp.maximum(logs[0], logs[1]), jnp.maximum(logs[2], logs[3]))
    parts = [jnp.exp2(v - top) for v in logs]
    inv = 1.0 / (parts[0] + parts[1] + parts[2] + parts[3])
    for i in range(NY):
        scaled = parts[i] * inv
        wcols[i] = jnp.concatenate([scaled, scaled], axis=0).T
    first_row = pl.multiple_of((x % 2) * 64, 64)
    shares = [wcols[i, pl.ds(first_row, 64), :] for i in range(NY)]
    for n in range(HEADS):
        lane = (n // 2) * 8 + n % 2
        cols = slice(n * 128, (n + 1) * 128)
        half = slice(n % 2 * 128, n % 2 * 128 + 128)
        mixed = shares[0][:, lane : lane + 1] * rbuf[0, n // 2, :, half].astype(jnp.float32)
        for i in range(1, NY):
            mixed = mixed + shares[i][:, lane : lane + 1] * rbuf[i, n // 2, :, half].astype(
                jnp.float32
            )
        att[:, cols] = mixed.astype(jnp.bfloat16)

    pltpu.make_async_copy(w_in, wbuf.at[x], local_sem.at[5]).wait()
    pltpu.make_async_copy(res_in, res_ref, local_sem.at[8]).wait()
    pltpu.make_async_copy(gain_in, gain_ref, local_sem.at[9]).wait()
    for copy in partner_copies:
        copy.wait_recv()

    width = w_in.shape[1]
    chunk = 256

    def project(i, total):
        cols = pl.ds(pl.multiple_of(i * chunk, chunk), chunk)
        part = jnp.dot(att[:, 0:512], wbuf[0, :, cols], preferred_element_type=jnp.float32)
        for b in range(1, NX):
            part = part + jnp.dot(
                att[:, b * 512 : (b + 1) * 512],
                wbuf[b, :, cols],
                preferred_element_type=jnp.float32,
            )
        stream = (res_ref[:, cols].astype(jnp.float32) + part).astype(jnp.bfloat16)
        stream_ref[:, cols] = stream
        wide = stream.astype(jnp.float32)
        return total + jnp.sum(wide * wide, axis=1, keepdims=True)

    total = lax.fori_loop(0, width // chunk, project, jnp.zeros((64, 1), jnp.float32))
    rate = lax.rsqrt(total * (1.0 / width) + norm_eps)
    normed_ref[...] = (stream_ref[...].astype(jnp.float32) * rate * gain_ref[...]).astype(
        jnp.bfloat16
    )

    for copy in first_sends + forwards + w_share + w_first + w_forward + spread_copies + partner_copies:
        copy.wait_send()

    def wait_q(i, _):
        for copy in q_copies(i + 1):
            copy.wait_send()
        return 0

    lax.fori_loop(0, 7, wait_q, 0)

    def wait_sent(r, _):
        for copy in o_copy((r + 1) // NX, (r + 1) % NX):
            copy.wait_send()
        return 0

    lax.fori_loop(0, 31, wait_sent, 0)


def experts_parts(
    normed_ref,
    stream_ref,
    ids_ref,
    route_ref,
    eg_in,
    eu_in,
    ed_in,
    sg_in,
    su_in,
    sd_in,
    out_ref,
    nbuf,
    table,
    tables,
    sel,
    gate,
    sbuf,
    xbuf,
    obuf,
    rbuf,
    cin,
    cout,
    total,
    eg,
    eu,
    ed,
    sg,
    su,
    sd,
    n_send,
    n_recv,
    t_send,
    t_recv,
    x_send,
    x_recv,
    r_send,
    r_recv,
    c_send,
    c_recv,
    w_sem,
    x_sem,
    r_sem,
):
    sp = lax.axis_index("sp")
    x = lax.axis_index("tp")
    z = sp // 8
    me8 = sp % 8
    zbase = z * 8
    width = normed_ref.shape[1]
    half = width // 2

    def at_z(step):
        return ((z + step + NZ) % NZ) * 8 + me8

    loads = [
        pltpu.make_async_copy(src, dst, w_sem.at[i])
        for i, (src, dst) in enumerate(
            (
                (sg_in, sg),
                (su_in, su),
                (sd_in, sd),
                (eg_in.at[0], eg),
                (eu_in.at[0], eu),
                (ed_in.at[0], ed),
            )
        )
    ]
    def remote(src, dst, send, recv, sp_id):
        return pltpu.make_async_remote_copy(
            src_ref=src,
            dst_ref=dst,
            send_sem=send,
            recv_sem=recv,
            device_id=(sp_id, x),
            device_id_type=MESH,
        )

    def pass_on(slot, to_slot, hf, step):
        return remote(
            nbuf.at[slot, hf],
            nbuf.at[to_slot, hf],
            n_send.at[to_slot, hf],
            n_recv.at[to_slot, hf],
            at_z(step),
        )

    sent = []

    def send(copy):
        copy.start()
        sent.append(copy)

    f32, bf16 = jnp.float32, jnp.bfloat16
    up, down = 1, 1 + UP_STEPS

    def table_copy(r):
        to = (z + r) % NZ
        return remote(table.at[to], tables.at[z], t_send.at[r], t_recv.at[r], to * 8 + me8)

    def prepare():
        for copy in loads:
            copy.start()

        both = jnp.concatenate([ids_ref[...].astype(f32), route_ref[...]], axis=0)
        both = jnp.concatenate([both, jnp.zeros_like(both)], axis=1)
        columns = jnp.concatenate([both] * 16, axis=0).T
        rows = ids_ref.shape[1]
        ids = columns[:rows, :TOPK]
        weights = columns[:rows, TOPK : 2 * TOPK]
        gates = weights / jnp.sum(weights, axis=1, keepdims=True) * routed_scale
        experts = lax.broadcasted_iota(jnp.int32, (rows, 64), 1).astype(f32)
        named = jnp.zeros((rows, 64), f32)
        shares = jnp.zeros((rows, 64), f32)
        for k in range(TOPK):
            hit = ids[:, k : k + 1] == experts
            named = named + jnp.where(hit, 1.0, 0.0)
            shares = shares + jnp.where(hit, gates[:, k : k + 1], 0.0)
        earlier = (
            lax.broadcasted_iota(jnp.int32, (rows, rows), 1)
            < lax.broadcasted_iota(jnp.int32, (rows, rows), 0)
        )
        named = named.astype(bf16)
        rank = jnp.dot(jnp.where(earlier, 1.0, 0.0).astype(bf16), named, preferred_element_type=f32)
        lane = lax.broadcasted_iota(jnp.int32, (64, 1024), 1)
        expert = lax.broadcasted_iota(jnp.int32, (64, 1024), 0)
        spread = jnp.where(lane // 16 == expert, 1.0, 0.0).astype(bf16)
        named_x = jnp.dot(named, spread, preferred_element_type=f32)
        rank_x = jnp.dot(rank.astype(bf16), spread, preferred_element_type=f32)
        share_x = jnp.dot(shares.astype(bf16), spread, preferred_element_type=f32)
        want = (lax.broadcasted_iota(jnp.int32, (rows, 1024), 1) % 8).astype(f32)
        filled = jnp.where(rank_x == want, named_x, 0.0)
        token = lax.broadcasted_iota(jnp.int32, (rows, 1024), 0).astype(f32)
        source = jnp.sum(filled * (token + 1000.0), axis=0, keepdims=True) - 1000.0
        share = jnp.sum(filled * share_x, axis=0, keepdims=True)
        for p in range(NZ):
            lanes = slice(p * 128, (p + 1) * 128)
            table[p] = jnp.concatenate(
                [source[:, lanes], share[:, lanes], jnp.zeros((6, 128), f32)], axis=0
            )
        tables[z] = table[z]

        for r in range(1, NZ):
            send(table_copy(r))

    def main():
        nbuf[0, 0] = normed_ref[:, :half]
        nbuf[0, 1] = normed_ref[:, half:]
        for hf in (0, 1):
            send(pass_on(0, up, hf, 1))
            send(pass_on(0, down, hf, -1))

        for copy in loads[:3]:
            copy.wait()
        n = normed_ref[...]
        g = jnp.dot(n, sg[...], preferred_element_type=f32)
        u = jnp.dot(n, su[...], preferred_element_type=f32)
        hidden = (g / (1.0 + jnp.exp(-g)) * u).astype(bf16)
        for i in range(4):
            cols = slice(i * width // 4, (i + 1) * width // 4)
            total[:, cols] = stream_ref[:, cols].astype(f32) + jnp.dot(
                hidden, sd[:, cols], preferred_element_type=f32
            )

        pairs = ((1, 5), (2, 6), (3, 7), (4, 0))
        offset = {0: 0, 1: -1, 2: -2, 3: -3, 4: -4, 5: 1, 6: 2, 7: 3}

        def arrive(slot, step, send_on, hf):
            if slot == UP_STEPS:
                pass_on(3 if hf == 0 else 7, slot, hf, 1 if hf == 0 else -1).wait_recv()
                return
            pass_on(slot - 1 if slot not in (up, down) else 0, slot, hf, step).wait_recv()
            if slot in (3, 7):
                if hf == (0 if slot == 3 else 1):
                    send(pass_on(slot, UP_STEPS, hf, step))
            elif send_on:
                send(pass_on(slot, slot + 1, hf, step))

        def x_copy(b, hf, r):
            to = (me8 + r) % 8
            return remote(
                sbuf.at[b, hf, to], xbuf.at[b, hf, me8], x_send.at[b, hf, r], x_recv.at[b, hf, r], zbase + to
            )

        def r_copy(b, hf, r):
            to = (me8 + r) % 8
            return remote(
                obuf.at[b, hf, to], rbuf.at[b, hf, me8], r_send.at[b, hf, r], r_recv.at[b, hf, r], zbase + to
            )

        def x_own(b, hf):
            return pltpu.make_async_copy(sbuf.at[b, hf, me8], xbuf.at[b, hf, me8], x_sem.at[b, hf])

        def r_own(b, hf):
            return pltpu.make_async_copy(obuf.at[b, hf, me8], rbuf.at[b, hf, me8], r_sem.at[b, hf])

        def choose(b):
            first, second = pairs[b]
            ta = tables[(z + offset[first] + NZ) % NZ]
            tb = tables[(z + offset[second] + NZ) % NZ]
            lane_of = lax.broadcasted_iota(jnp.int32, (1, 128), 1) % 16
            src = jnp.where(lane_of < 8, ta[0:1], tb[0:1] + 64.0)
            share_row = jnp.where(lane_of < 8, ta[1:2], tb[1:2])
            token_of = lax.broadcasted_iota(jnp.int32, (128, 128), 0).astype(f32)
            chosen = jnp.where(token_of == src, 1.0, 0.0)
            sel[...] = chosen.T.astype(bf16)
            gate[b] = (chosen * share_row).astype(bf16)

        def dispatch(b, hf):
            first, second = pairs[b]
            for i in range(2):
                cols = slice(i * half // 2, (i + 1) * half // 2)
                tokens = jnp.concatenate([nbuf[first, hf, :, cols], nbuf[second, hf, :, cols]], axis=0)
                picked = jnp.dot(sel[...], tokens, preferred_element_type=f32)
                sbuf[b, hf, :, :, cols] = picked.astype(bf16).reshape(8, 16, half // 2)
            for r in (4, 3, 5, 2, 6, 1, 7):
                send(x_copy(b, hf, r))
            x_own(b, hf).start()

        def give_back(b, hf):
            for r in (4, 3, 5, 2, 6, 1, 7):
                send(r_copy(b, hf, r))
            r_own(b, hf).start()

        def run_expert(b, give):
            g = u = None
            for hf in (0, 1):
                for r in range(1, 8):
                    x_copy(b, hf, r).wait_recv()
                x_own(b, hf).wait()
                rows_in = xbuf[b, hf].reshape(128, half)
                deep = slice(hf * half, (hf + 1) * half)
                g_part = jnp.dot(rows_in, eg[deep, :], preferred_element_type=f32)
                u_part = jnp.dot(rows_in, eu[deep, :], preferred_element_type=f32)
                g = g_part if g is None else g + g_part
                u = u_part if u is None else u + u_part
            hidden = (g / (1.0 + jnp.exp(-g)) * u).astype(bf16)
            for hf in (0, 1):
                for i in range(2):
                    cols = slice(i * half // 2, (i + 1) * half // 2)
                    at = hf * half + i * half // 2
                    made = jnp.dot(hidden, ed[:, at : at + half // 2], preferred_element_type=f32)
                    obuf[b, hf, :, :, cols] = made.astype(bf16).reshape(8, 16, half // 2)
                if give:
                    give_back(b, hf)

        def need_tables(*steps):
            for r in steps:
                table_copy(r).wait_recv()

        for b, moves, steps in (
            (0, ((1, 1, True), (5, -1, True)), (1, 7)),
            (1, ((2, 1, True), (6, -1, True)), (2, 6)),
            (2, ((3, 1, True), (7, -1, True)), (3, 5)),
            (3, ((4, 1, False),), (4,)),
        ):
            for hf in (0, 1):
                for slot, step, send_on in moves:
                    arrive(slot, step, send_on, hf)
                if hf == 0:
                    need_tables(*steps)
                    choose(b)
                dispatch(b, hf)
            if b == 0:
                for copy in loads[3:]:
                    copy.wait()
            else:
                run_expert(b - 1, False)
        run_expert(3, True)
        for b in (2, 1, 0):
            for hf in (0, 1):
                give_back(b, hf)

        def chain_copy(way, place, hf):
            return remote(
                cout.at[way, place, hf],
                cin.at[way, place, hf],
                c_send.at[way, place, hf],
                c_recv.at[way, place, hf],
                at_z(-1 if way == 0 else 1),
            )

        for b, places in ((3, (3, None)), (2, (2, 2)), (1, (1, 1)), (0, (0, 0))):
            for hf in (0, 1):
                for r in range(1, 8):
                    r_copy(b, hf, r).wait_recv()
                r_own(b, hf).wait()
                cols = slice(hf * half, (hf + 1) * half)
                part = jnp.dot(
                    gate[b], rbuf[b, hf].reshape(128, half), preferred_element_type=f32
                )
                for way in (0, 1):
                    mine = part[way * 64 : (way + 1) * 64]
                    place = places[way]
                    if place is None:
                        total[:, cols] = total[:, cols] + mine
                        continue
                    side = way if place < 3 else hf
                    if place < 2 or (place == 2 and hf == way):
                        chain_copy(side, place + 1, hf).wait_recv()
                        mine = mine + cin[side, place + 1, hf].astype(f32)
                    cout[side, place, hf] = mine.astype(bf16)
                    send(chain_copy(side, place, hf))
        for hf in (0, 1):
            cols = slice(hf * half, (hf + 1) * half)
            for way in (0, 1):
                chain_copy(way, 0, hf).wait_recv()
            out_ref[:, cols] = (
                total[:, cols] + cin[0, 0, hf].astype(f32) + cin[1, 0, hf].astype(f32)
            ).astype(bf16)
        for copy in sent:
            copy.wait_send()

    return prepare, main


def layer_kernel(*refs):
    att_in, (ids, route), weights = refs[:7], refs[7:9], refs[9:15]
    out, stream, normed = refs[15:18]
    att_scratch, scratch = refs[18 : 18 + ATTENTION_SCRATCH], refs[18 + ATTENTION_SCRATCH :]
    prepare, main = experts_parts(normed, stream, ids, route, *weights, out, *scratch)
    attention_kernel(prepare, *att_in, stream, normed, *att_scratch)
    main()


ATTENTION_SCRATCH = 36


def layer(
    residual,
    queries,
    key_rows,
    value_rows,
    forget_sums,
    out_weight,
    norm_gain,
    expert_ids,
    route_weights,
    expert_gate,
    expert_up,
    expert_down,
    shared_gate,
    shared_up,
    shared_down,
):
    rows, width = residual.shape
    tokens = queries.shape[0]
    hidden = expert_gate.shape[2]
    shared = shared_gate.shape[1]
    q_in = queries.T.reshape(2, 256, tokens)
    v_in = value_rows.T.reshape(2, 128, tokens)
    bf16, f32 = jnp.bfloat16, jnp.float32
    anywhere = pl.BlockSpec(memory_space=pl.ANY)
    vmem = pl.BlockSpec(memory_space=pltpu.VMEM)
    dma = pltpu.SemaphoreType.DMA
    return pl.pallas_call(
        layer_kernel,
        out_shape=jax.ShapeDtypeStruct((rows, width), bf16),
        in_specs=[anywhere, anywhere, anywhere, vmem] + [anywhere] * 3 + [vmem] * 2 + [anywhere] * 6,
        out_specs=vmem,
        scratch_shapes=[
            pltpu.VMEM((rows, width), bf16),
            pltpu.VMEM((rows, width), bf16),
            pltpu.VMEM((8, 256, 256), bf16),
            pltpu.VMEM((8, 8, 256), f32),
            pltpu.VMEM((8, 2, 256, 128), bf16),
            pltpu.VMEM((8, 2, 128, 256), bf16),
            pltpu.VMEM((8, 2, 8, 256), f32),
            pltpu.VMEM((2, 8, 256), f32),
            pltpu.VMEM((8, 2, 256, 128), bf16),
            pltpu.VMEM((2, 128, 256), bf16),
            pltpu.VMEM((2, 2, 256, 256), f32),
            pltpu.VMEM((2, 2, 256, 256), f32),
            pltpu.VMEM((64, 2048), bf16),
            pltpu.VMEM((1, 2048), f32),
            pltpu.VMEM((8, 2, 128, 256), f32),
            pltpu.VMEM((8, 8, 256), f32),
            pltpu.VMEM((8, 256, 256), bf16),
            pltpu.VMEM((8, 2, 8, 128), f32),
            pltpu.VMEM((4, 8, 64, 256), bf16),
            pltpu.VMEM((4, 8, 8, 128), f32),
            pltpu.VMEM((4, 128, 128), f32),
            pltpu.VMEM((64, 2048), bf16),
            pltpu.VMEM((4, 512, 2048), bf16),
            dma((2, 8)),
            dma((2, 8)),
            dma((3, 8, 2)),
            dma((3, 8, 2)),
            dma((8, 4)),
            dma((8, 4)),
            dma((8, 4)),
            dma((8, 4)),
            dma((9,)),
            dma((9,)),
            dma((3, NY)),
            dma((3, NY)),
            dma((3, 2)),
            dma((3, 2)),
            dma((10,)),
            pltpu.VMEM((8, 2, rows, width // 2), bf16),
            pltpu.VMEM((8, 8, 128), f32),
            pltpu.VMEM((8, 8, 128), f32),
            pltpu.VMEM((128, 128), bf16),
            pltpu.VMEM((4, 128, 128), bf16),
            pltpu.VMEM((4, 2, 8, 16, width // 2), bf16),
            pltpu.VMEM((4, 2, 8, 16, width // 2), bf16),
            pltpu.VMEM((4, 2, 8, 16, width // 2), bf16),
            pltpu.VMEM((4, 2, 8, 16, width // 2), bf16),
            pltpu.VMEM((2, 4, 2, rows, width // 2), bf16),
            pltpu.VMEM((2, 4, 2, rows, width // 2), bf16),
            pltpu.VMEM((rows, width), f32),
            pltpu.VMEM((width, hidden), bf16),
            pltpu.VMEM((width, hidden), bf16),
            pltpu.VMEM((hidden, width), bf16),
            pltpu.VMEM((width, shared), bf16),
            pltpu.VMEM((width, shared), bf16),
            pltpu.VMEM((shared, width), bf16),
            dma((8, 2)),
            dma((8, 2)),
            dma((8,)),
            dma((8,)),
            dma((4, 2, 8)),
            dma((4, 2, 8)),
            dma((4, 2, 8)),
            dma((4, 2, 8)),
            dma((2, 4, 2)),
            dma((2, 4, 2)),
            dma((6,)),
            dma((4, 2)),
            dma((4, 2)),
        ],
        compiler_params=pltpu.CompilerParams(
            collective_id=0, has_side_effects=True, vmem_limit_bytes=66_000_000
        ),
        cost_estimate=pl.CostEstimate(
            flops=12 * 10**9, bytes_accessed=32 * 2**20, transcendentals=16 * 2**20
        ),
    )(
        q_in,
        key_rows,
        v_in,
        forget_sums.T,
        out_weight,
        residual,
        norm_gain.reshape(1, width),
        expert_ids.T,
        route_weights.T,
        expert_gate,
        expert_up,
        expert_down,
        shared_gate,
        shared_up,
        shared_down,
    )


def solution(mesh):
    in_specs = (
        P(("sp", "tp"), None),
        P("sp", "tp"),
        P("sp", "tp"),
        P("sp", "tp"),
        P("sp", "tp"),
        P("tp", None),
        P(),
        P(("sp", "tp"), None),
        P(("sp", "tp"), None),
        P("sp", None, None),
        P("sp", None, None),
        P("sp", None, None),
        P(),
        P(),
        P(),
    )
    out_specs = P(("sp", "tp"), None)
    return jax.shard_map(layer, mesh=mesh, in_specs=in_specs, out_specs=out_specs, check_vma=False)
```

```python
import jax
import jax.numpy as jnp
from jax import lax
from jax.experimental import pallas as pl
from jax.experimental.pallas import tpu as pltpu
from jax.sharding import PartitionSpec as P

HEADS = 16
KV_HEADS = 8
HEAD_DIM = 128
TOPK = 4
MESH = pl.DeviceIdType.MESH
LOG2E = 1.4426950408889634
NEG = -1e30

routed_scale = 2.5
norm_eps = 1e-06

NZ, NY, NX = 8, 4, 4
UP_STEPS, DOWN_STEPS = 4, 3


def attention_kernel(
    prepare,
    q_rows,
    k_rows,
    v_rows,
    f_rows,
    w_in,
    res_in,
    gain_in,
    stream_ref,
    normed_ref,
    q_in,
    v_in,
    qbuf,
    fqbuf,
    kbuf,
    vbuf,
    fbuf,
    f_in,
    bias,
    ones,
    held_a,
    held_b,
    res_ref,
    gain_ref,
    acc,
    stats,
    obuf,
    lbuf,
    rbuf,
    lrecv,
    wcols,
    att,
    wbuf,
    q_send,
    q_recv,
    kv_send,
    kv_recv,
    o_send,
    o_recv,
    l_send,
    l_recv,
    w_send,
    w_recv,
    s_send,
    s_recv,
    p_send,
    p_recv,
    local_sem,
):
    sp = lax.axis_index("sp")
    x = lax.axis_index("tp")
    z = sp // 8
    me8 = sp % 8
    y = me8 // 2
    c = me8 % 2
    zbase = z * 8

    def at_z(step, core):
        return ((z + step + NZ) % NZ) * 8 + y * 2 + core

    partner = zbase + y * 2 + (1 - c)
    xr = (x + 1) % NX
    xl = (x + NX - 1) % NX

    barrier = pltpu.get_barrier_semaphore()

    def greet_plane(i, _):
        n = i + 1
        r8, rx = n // NX, n % NX
        pl.semaphore_signal(
            barrier,
            inc=1,
            device_id=(zbase + (me8 + r8) % 8, (x + rx) % NX),
            device_id_type=MESH,
        )
        return 0

    lax.fori_loop(0, 31, greet_plane, 0)
    for step in range(2, NZ - 1):
        pl.semaphore_signal(barrier, inc=1, device_id=(at_z(step, c), x), device_id_type=MESH)
    for step in (1, -1):
        for core in (0, 1):
            pl.semaphore_signal(
                barrier, inc=1, device_id=(at_z(step, core), x), device_id_type=MESH
            )
    pltpu.make_async_copy(w_in, wbuf.at[x], local_sem.at[5]).start()
    pltpu.make_async_copy(res_in, res_ref, local_sem.at[8]).start()
    pltpu.make_async_copy(gain_in, gain_ref, local_sem.at[9]).start()
    for h in (0, 1):
        q_in[h] = q_rows[:, h * 256 : (h + 1) * 256].T
        v_in[h] = v_rows[:, h * 128 : (h + 1) * 128].T
        f_in[h] = jnp.concatenate(
            [f_rows[2 * h : 2 * h + 2, :], jnp.zeros((6, f_rows.shape[1]), jnp.float32)], axis=0
        )
        row = lax.broadcasted_iota(jnp.int32, (128, 256), 0)
        ones[h] = jnp.where((row % 8 == h) & (row < 24), 1.0, 0.0).astype(jnp.bfloat16)
    acc[...] = jnp.zeros_like(acc)
    row = lax.broadcasted_iota(jnp.int32, stats.shape, 1)
    stats[...] = jnp.where(row < 2, NEG, 0.0)
    pl.semaphore_wait(barrier, 40)

    def remote(src, dst, send, recv, sp_id, tp_id):
        return pltpu.make_async_remote_copy(
            src_ref=src,
            dst_ref=dst,
            send_sem=send,
            recv_sem=recv,
            device_id=(sp_id, tp_id),
            device_id_type=MESH,
        )

    kv_arrays = ((k_rows, kbuf), (v_in, vbuf), (f_in, fbuf))

    def own_piece(a, h):
        if a == 0:
            return k_rows.at[:, pl.ds(pl.multiple_of(h * 128, 128), 128)]
        return kv_arrays[a][0].at[h]

    first_sends = []
    for a in (2, 0, 1):
        dst = kv_arrays[a][1]
        pltpu.make_async_copy(own_piece(a, c), dst.at[0, c], local_sem.at[a]).start()
        first_sends.append(
            remote(
                own_piece(a, 1 - c),
                dst.at[0, c],
                kv_send.at[a, 0, 0],
                kv_recv.at[a, 0, 0],
                partner,
                x,
            )
        )
        for step, slot in ((1, 1), (-1, 1 + UP_STEPS)):
            for h in (0, 1):
                first_sends.append(
                    remote(
                        own_piece(a, h),
                        dst.at[slot, c],
                        kv_send.at[a, slot, h],
                        kv_recv.at[a, slot, c],
                        at_z(step, h),
                        x,
                    )
                )
    for copy in first_sends:
        copy.start()

    pltpu.make_async_copy(q_in.at[c], qbuf.at[me8], local_sem.at[3]).start()
    pltpu.make_async_copy(f_in.at[c], fqbuf.at[me8], local_sem.at[4]).start()

    def q_copies(r):
        to = (me8 + r) % 8
        return (
            remote(f_in.at[to % 2], fqbuf.at[me8], q_send.at[1, r], q_recv.at[1, r], zbase + to, x),
            remote(q_in.at[to % 2], qbuf.at[me8], q_send.at[0, r], q_recv.at[0, r], zbase + to, x),
        )

    def start_q(i, _):
        for copy in q_copies(i + 1):
            copy.start()
        return 0

    lax.fori_loop(0, 7, start_q, 0)

    mine = w_in.shape[0] // 2
    shared_rows = mine // 4
    part = shared_rows // NY
    direct = mine - shared_rows
    eighth = direct // 2
    top_row = c * mine
    rows_a = pl.ds(top_row, direct)
    rows_a0 = pl.ds(top_row, eighth)
    rows_a1 = pl.ds(top_row + eighth, eighth)
    rows_b = pl.ds(top_row + direct, shared_rows)
    across = (x + 2) % NX
    others = (xl, xr, across)

    def share_rows(yy):
        return pl.ds(top_row + direct + yy * part, part)

    def x_of(i, step):
        return (x + step * (1, -1, 2)[i] + NX) % NX

    w_share = [
        remote(
            w_in.at[share_rows(y)], wbuf.at[x, share_rows(y)], w_send.at[i], w_recv.at[i], sp, x_of(i, 1)
        )
        for i in range(3)
    ]
    w_first = [
        remote(w_in.at[rows_a0], wbuf.at[x, rows_a0], w_send.at[3], w_recv.at[3], sp, xr),
        remote(w_in.at[rows_a1], wbuf.at[x, rows_a1], w_send.at[4], w_recv.at[4], sp, xl),
        remote(w_in.at[rows_a1], wbuf.at[x, rows_a1], w_send.at[5], w_recv.at[5], sp, xr),
        remote(w_in.at[rows_a0], wbuf.at[x, rows_a0], w_send.at[6], w_recv.at[6], sp, xl),
    ]
    for copy in w_share + w_first:
        copy.start()
    w_forward = [
        remote(wbuf.at[xl, rows_a0], wbuf.at[xl, rows_a0], w_send.at[7], w_recv.at[7], sp, xr),
        remote(wbuf.at[xr, rows_a1], wbuf.at[xr, rows_a1], w_send.at[8], w_recv.at[8], sp, xl),
    ]
    w_spread = [
        [
            remote(
                wbuf.at[o, share_rows(y)],
                wbuf.at[o, share_rows(y)],
                s_send.at[i, dy],
                s_recv.at[i, dy],
                zbase + ((y + dy) % NY) * 2 + c,
                x,
            )
            for dy in range(1, NY)
        ]
        for i, o in enumerate(others)
    ]
    w_partner = [
        [
            remote(wbuf.at[o, rows], wbuf.at[o, rows], p_send.at[i, k], p_recv.at[i, k], partner, x)
            for k, rows in enumerate((rows_a, rows_b))
        ]
        for i, o in enumerate(others)
    ]
    partner_copies = [copy for row in w_partner for copy in row]
    spread_copies = [copy for row in w_spread for copy in row]

    prepare()

    scale = HEAD_DIM ** (-0.5) * LOG2E
    root = HEAD_DIM**0.5

    def make_bias(slot):
        f0 = fbuf[slot, 0]
        base = f0[:, 0:1]
        for cc in (0, 1):
            rest = (base - (f0 if cc == 0 else fbuf[slot, 1])) * root
            pieces = []
            for _ in range(3):
                piece = rest.astype(jnp.bfloat16).astype(jnp.float32)
                pieces.append(piece)
                rest = rest - piece
            pieces.append(jnp.zeros((104, 256), jnp.float32))
            bias[slot, cc] = jnp.concatenate(pieces, axis=0).T.astype(jnp.bfloat16)

    def score(slot, qb, h, cc):
        q_h = jnp.concatenate([qbuf[qb, h * 128 : (h + 1) * 128, :], ones[h]], axis=0)
        keys = jnp.concatenate([kbuf[slot, cc], bias[slot, cc]], axis=1)
        return jnp.dot(keys, q_h, preferred_element_type=jnp.float32)

    span = 64

    def weigh(slot, qb, h, held):
        delta = (fqbuf[qb, h : h + 1, 0:1] - fbuf[slot, 0, h : h + 1, 0:1]) * root
        pieces = [(cc, slice(r, r + span)) for cc in (0, 1) for r in range(0, 256, span)]
        top = None
        for cc, part in pieces:
            high = jnp.max(held[h, cc, part, :].reshape(span // 8, 8, 256), axis=0)
            top = high if top is None else jnp.maximum(top, high)
        top = jnp.max(top, axis=0, keepdims=True)
        old = stats[qb, h : h + 1, :]
        new = jnp.maximum(old, top + delta)
        shift = new - delta
        factor = jnp.exp2((old - new) * scale)
        total = jnp.zeros((8, 256), jnp.float32)
        p = ([], [])
        for cc, part in pieces:
            e = jnp.exp2((held[h, cc, part, :] - shift) * scale)
            total = total + jnp.sum(e.reshape(span // 8, 8, 256), axis=0)
            p[cc].append(e.astype(jnp.bfloat16))
        total = jnp.sum(total, axis=0, keepdims=True)
        stats[qb, h : h + 1, :] = new
        stats[qb, 2 + h : 3 + h, :] = stats[qb, 2 + h : 3 + h, :] * factor + total
        mixed = jnp.dot(
            vbuf[slot, 0], jnp.concatenate(p[0], axis=0), preferred_element_type=jnp.float32
        ) + jnp.dot(vbuf[slot, 1], jnp.concatenate(p[1], axis=0), preferred_element_type=jnp.float32)
        acc[qb, h] = acc[qb, h] * factor + mixed

    def own_task(qb):
        rows = lax.broadcasted_iota(jnp.int32, (256, 256), 0)
        cols = lax.broadcasted_iota(jnp.int32, (256, 256), 1)
        gap = (qb - 2 * y) * 256
        for h in (0, 1):
            for cc in (0, 1):
                held_a[h, cc] = jnp.where(
                    rows + cc * 256 <= cols + gap, score(0, qb, h, cc), -jnp.inf
                )
        use(held_a, 0, qb)

    def fill(held, slot, qb):
        for h in (0, 1):
            for cc in (0, 1):
                held[h, cc] = score(slot, qb, h, cc)

    def use(held, slot, qb):
        for h in (0, 1):
            weigh(slot, qb, h, held)

    def run_tasks(count, place, after=None):
        @pl.when(count > 0)
        def _():
            fill(held_a, *place(0))

        def pair(i, _):
            first, second = 2 * i, 2 * i + 1
            fill(held_b, *place(second))
            use(held_a, *place(first))
            if after is not None:
                after(first)
            fill(held_a, *place(jnp.minimum(second + 1, count - 1)))
            use(held_b, *place(second))
            if after is not None:
                after(second)
            return 0

        lax.fori_loop(0, count // 2, pair, 0)

    def wait_first(a, slot):
        for h in (0, 1):
            remote(
                own_piece(a, h),
                kv_arrays[a][1].at[slot, h],
                kv_send.at[a, slot, h],
                kv_recv.at[a, slot, h],
                partner,
                x,
            ).wait_recv()

    def forward(a, slot, step):
        buf = kv_arrays[a][1]
        if slot in (UP_STEPS - 1, UP_STEPS + DOWN_STEPS):
            piece = 0 if slot == UP_STEPS - 1 else 1
            return remote(
                buf.at[slot, piece],
                buf.at[UP_STEPS, piece],
                kv_send.at[a, UP_STEPS, piece],
                kv_recv.at[a, UP_STEPS, piece],
                at_z(step, c),
                x,
            )
        return remote(
            buf.at[slot],
            buf.at[slot + 1],
            kv_send.at[a, slot + 1, 0],
            kv_recv.at[a, slot + 1, 0],
            at_z(step, c),
            x,
        )

    forwards = []

    def arrive(slot, step, first, send_on):
        for a in (2, 0, 1):
            if first:
                wait_first(a, slot)
            else:
                forward(a, slot - 1, step).wait_recv()
            if send_on:
                copy = forward(a, slot, step)
                copy.start()
                forwards.append(copy)

    def valid(j):
        return jnp.where(z >= j, 1, 0) + jnp.where(z >= NZ - j, 1, 0)

    def peer(i):
        return jnp.where(i % 2 == 1, (i + 1) // 2, (8 - i // 2) % 8)

    def block_of(i):
        return (me8 + 8 - peer(i)) % 8

    def wait_query(i):
        @pl.when(i > 0)
        def _():
            for copy in q_copies(jnp.maximum(peer(i), 1)):
                copy.wait_recv()

    def own(i):
        wait_query(i)
        qb = block_of(i)

        @pl.when(qb // 2 >= y)
        def _():
            own_task(qb)

    for a in range(3):
        pltpu.make_async_copy(own_piece(a, c), kv_arrays[a][1].at[0, c], local_sem.at[a]).wait()
        remote(
            own_piece(a, 1 - c),
            kv_arrays[a][1].at[0, c],
            kv_send.at[a, 0, 0],
            kv_recv.at[a, 0, 0],
            partner,
            x,
        ).wait_recv()
    pltpu.make_async_copy(q_in.at[c], qbuf.at[me8], local_sem.at[3]).wait()
    pltpu.make_async_copy(f_in.at[c], fqbuf.at[me8], local_sem.at[4]).wait()
    make_bias(0)

    near = 4

    def stage_a(i, _):
        own(i)
        return 0

    lax.fori_loop(0, near, stage_a, 0)
    arrive(1, 1, True, True)
    arrive(5, -1, True, True)
    for i in range(3):
        w_share[i].wait_recv()
        for copy in w_spread[i]:
            copy.start()
    make_bias(1)
    make_bias(5)

    run_tasks(near * valid(1), lambda t: (1 + 4 * (t // near), block_of(t % near)))
    arrive(2, 1, False, True)
    arrive(6, -1, False, True)
    make_bias(2)
    make_bias(6)
    w_first[0].wait_recv()
    w_forward[0].start()
    w_first[1].wait_recv()
    w_forward[1].start()

    lax.fori_loop(near, 8, stage_a, 0)
    run_tasks(near * valid(1), lambda t: (1 + 4 * (t // near), block_of(near + t % near)))
    arrive(3, 1, False, True)
    arrive(7, -1, False, True)
    make_bias(3)
    make_bias(7)
    run_tasks(8 * valid(2), lambda t: (2 + 4 * (t // 8), block_of(t % 8)))
    w_first[2].wait_recv()
    w_first[3].wait_recv()
    w_partner[0][0].start()
    w_partner[1][0].start()
    run_tasks(8 * valid(3), lambda t: (3 + 4 * (t // 8), block_of(t % 8)))
    w_forward[0].wait_recv()
    w_forward[1].wait_recv()
    w_partner[2][0].start()
    for a in (2, 0, 1):
        forward(a, 3, 1).wait_recv()
        forward(a, 7, -1).wait_recv()
    make_bias(4)

    def o_copy(r8, rx):
        to = (me8 + r8) % 8
        tx = (x + rx) % NX
        return (
            remote(
                obuf.at[to, pl.ds(tx * 64, 64)],
                rbuf.at[y, x * 2 + c],
                o_send.at[r8, rx],
                o_recv.at[r8, rx],
                zbase + to,
                tx,
            ),
            remote(
                lbuf.at[to, tx // 2],
                lrecv.at[y, x * 2 + c],
                l_send.at[r8, rx],
                l_recv.at[r8, rx],
                zbase + to,
                tx,
            ),
        )

    def finish(r):
        i = 7 - r
        qb = block_of(i)
        r8 = (8 - peer(i)) % 8
        sums = []
        for h in (0, 1):
            total = stats[qb, 2 + h : 3 + h, :]
            some = total > 0.0
            inv = jnp.where(some, 1.0 / jnp.where(some, total, 1.0), 0.0)
            obuf[qb, :, h * 128 : (h + 1) * 128] = (acc[qb, h] * inv).T.astype(jnp.bfloat16)
            sums.append(
                jnp.where(
                    some, stats[qb, h : h + 1, :] * scale + jnp.log2(jnp.where(some, total, 1.0)), NEG
                )
            )
        both = jnp.concatenate(sums + [jnp.zeros((6, 256), jnp.float32)], axis=0)
        lbuf[qb, 0] = both[:, :128]
        lbuf[qb, 1] = both[:, 128:]
        for rx in (2, 1, 3):
            for copy in o_copy(r8, rx):
                copy.start()

        @pl.when(r8 > 0)
        def _():
            for copy in o_copy(r8, 0):
                copy.start()

    last = jnp.where(z >= UP_STEPS, 1, 0)

    def last_place(t):
        return UP_STEPS, block_of(7 - t)

    def leave(t):
        finish(t)

    run_tasks(8 * last, last_place, leave)

    def finish_early(r, _):
        finish(r)
        return 0

    lax.fori_loop(0, jnp.where(last == 0, 8, 0), finish_early, 0)
    for copy in spread_copies:
        copy.wait_recv()
    for row in w_partner:
        row[1].start()
    own_copies = (
        pltpu.make_async_copy(
            obuf.at[me8, pl.ds(x * 64, 64)],
            rbuf.at[y, x * 2 + c],
            local_sem.at[6],
        ),
        pltpu.make_async_copy(lbuf.at[me8, x // 2], lrecv.at[y, x * 2 + c], local_sem.at[7]),
    )
    for copy in own_copies:
        copy.start()
    for copy in own_copies:
        copy.wait()

    def wait_o(r, _):
        for copy in o_copy((r + 1) // NX, (r + 1) % NX):
            copy.wait_recv()
        return 0

    lax.fori_loop(0, 31, wait_o, 0)

    logs = [lrecv[i].reshape(64, 128) for i in range(NY)]
    top = jnp.maximum(jnp.maximum(logs[0], logs[1]), jnp.maximum(logs[2], logs[3]))
    parts = [jnp.exp2(v - top) for v in logs]
    inv = 1.0 / (parts[0] + parts[1] + parts[2] + parts[3])
    for i in range(NY):
        scaled = parts[i] * inv
        wcols[i] = jnp.concatenate([scaled, scaled], axis=0).T
    first_row = pl.multiple_of((x % 2) * 64, 64)
    shares = [wcols[i, pl.ds(first_row, 64), :] for i in range(NY)]
    for n in range(HEADS):
        lane = (n // 2) * 8 + n % 2
        cols = slice(n * 128, (n + 1) * 128)
        half = slice(n % 2 * 128, n % 2 * 128 + 128)
        mixed = shares[0][:, lane : lane + 1] * rbuf[0, n // 2, :, half].astype(jnp.float32)
        for i in range(1, NY):
            mixed = mixed + shares[i][:, lane : lane + 1] * rbuf[i, n // 2, :, half].astype(
                jnp.float32
            )
        att[:, cols] = mixed.astype(jnp.bfloat16)

    pltpu.make_async_copy(w_in, wbuf.at[x], local_sem.at[5]).wait()
    pltpu.make_async_copy(res_in, res_ref, local_sem.at[8]).wait()
    pltpu.make_async_copy(gain_in, gain_ref, local_sem.at[9]).wait()
    for copy in partner_copies:
        copy.wait_recv()

    width = w_in.shape[1]
    chunk = 256

    def project(i, total):
        cols = pl.ds(pl.multiple_of(i * chunk, chunk), chunk)
        part = jnp.dot(att[:, 0:512], wbuf[0, :, cols], preferred_element_type=jnp.float32)
        for b in range(1, NX):
            part = part + jnp.dot(
                att[:, b * 512 : (b + 1) * 512],
                wbuf[b, :, cols],
                preferred_element_type=jnp.float32,
            )
        stream = (res_ref[:, cols].astype(jnp.float32) + part).astype(jnp.bfloat16)
        stream_ref[:, cols] = stream
        wide = stream.astype(jnp.float32)
        return total + jnp.sum(wide * wide, axis=1, keepdims=True)

    total = lax.fori_loop(0, width // chunk, project, jnp.zeros((64, 1), jnp.float32))
    rate = lax.rsqrt(total * (1.0 / width) + norm_eps)
    normed_ref[...] = (stream_ref[...].astype(jnp.float32) * rate * gain_ref[...]).astype(
        jnp.bfloat16
    )

    for copy in first_sends + forwards + w_share + w_first + w_forward + spread_copies + partner_copies:
        copy.wait_send()

    def wait_q(i, _):
        for copy in q_copies(i + 1):
            copy.wait_send()
        return 0

    lax.fori_loop(0, 7, wait_q, 0)

    def wait_sent(r, _):
        for copy in o_copy((r + 1) // NX, (r + 1) % NX):
            copy.wait_send()
        return 0

    lax.fori_loop(0, 31, wait_sent, 0)


def experts_parts(
    normed_ref,
    stream_ref,
    ids_ref,
    route_ref,
    eg_in,
    eu_in,
    ed_in,
    sg_in,
    su_in,
    sd_in,
    out_ref,
    nbuf,
    table,
    tables,
    sel,
    gate,
    sbuf,
    xbuf,
    obuf,
    rbuf,
    cin,
    cout,
    total,
    eg,
    eu,
    ed,
    sg,
    su,
    sd,
    n_send,
    n_recv,
    t_send,
    t_recv,
    x_send,
    x_recv,
    r_send,
    r_recv,
    c_send,
    c_recv,
    w_sem,
    x_sem,
    r_sem,
):
    sp = lax.axis_index("sp")
    x = lax.axis_index("tp")
    z = sp // 8
    me8 = sp % 8
    zbase = z * 8
    width = normed_ref.shape[1]
    half = width // 2

    def at_z(step):
        return ((z + step + NZ) % NZ) * 8 + me8

    loads = [
        pltpu.make_async_copy(src, dst, w_sem.at[i])
        for i, (src, dst) in enumerate(
            (
                (sg_in, sg),
                (su_in, su),
                (sd_in, sd),
                (eg_in.at[0], eg),
                (eu_in.at[0], eu),
                (ed_in.at[0], ed),
            )
        )
    ]
    def remote(src, dst, send, recv, sp_id):
        return pltpu.make_async_remote_copy(
            src_ref=src,
            dst_ref=dst,
            send_sem=send,
            recv_sem=recv,
            device_id=(sp_id, x),
            device_id_type=MESH,
        )

    def pass_on(slot, to_slot, hf, step):
        return remote(
            nbuf.at[slot, hf],
            nbuf.at[to_slot, hf],
            n_send.at[to_slot, hf],
            n_recv.at[to_slot, hf],
            at_z(step),
        )

    sent = []

    def send(copy):
        copy.start()
        sent.append(copy)

    f32, bf16 = jnp.float32, jnp.bfloat16
    up, down = 1, 1 + UP_STEPS

    def table_copy(r):
        to = (z + r) % NZ
        return remote(table.at[to], tables.at[z], t_send.at[r], t_recv.at[r], to * 8 + me8)

    def prepare():
        for copy in loads:
            copy.start()

        both = jnp.concatenate([ids_ref[...].astype(f32), route_ref[...]], axis=0)
        both = jnp.concatenate([both, jnp.zeros_like(both)], axis=1)
        columns = jnp.concatenate([both] * 16, axis=0).T
        rows = ids_ref.shape[1]
        ids = columns[:rows, :TOPK]
        weights = columns[:rows, TOPK : 2 * TOPK]
        gates = weights / jnp.sum(weights, axis=1, keepdims=True) * routed_scale
        experts = lax.broadcasted_iota(jnp.int32, (rows, 64), 1).astype(f32)
        named = jnp.zeros((rows, 64), f32)
        shares = jnp.zeros((rows, 64), f32)
        for k in range(TOPK):
            hit = ids[:, k : k + 1] == experts
            named = named + jnp.where(hit, 1.0, 0.0)
            shares = shares + jnp.where(hit, gates[:, k : k + 1], 0.0)
        earlier = (
            lax.broadcasted_iota(jnp.int32, (rows, rows), 1)
            < lax.broadcasted_iota(jnp.int32, (rows, rows), 0)
        )
        named = named.astype(bf16)
        rank = jnp.dot(jnp.where(earlier, 1.0, 0.0).astype(bf16), named, preferred_element_type=f32)
        lane = lax.broadcasted_iota(jnp.int32, (64, 1024), 1)
        expert = lax.broadcasted_iota(jnp.int32, (64, 1024), 0)
        spread = jnp.where(lane // 16 == expert, 1.0, 0.0).astype(bf16)
        named_x = jnp.dot(named, spread, preferred_element_type=f32)
        rank_x = jnp.dot(rank.astype(bf16), spread, preferred_element_type=f32)
        share_x = jnp.dot(shares.astype(bf16), spread, preferred_element_type=f32)
        want = (lax.broadcasted_iota(jnp.int32, (rows, 1024), 1) % 8).astype(f32)
        filled = jnp.where(rank_x == want, named_x, 0.0)
        token = lax.broadcasted_iota(jnp.int32, (rows, 1024), 0).astype(f32)
        source = jnp.sum(filled * (token + 1000.0), axis=0, keepdims=True) - 1000.0
        share = jnp.sum(filled * share_x, axis=0, keepdims=True)
        for p in range(NZ):
            lanes = slice(p * 128, (p + 1) * 128)
            table[p] = jnp.concatenate(
                [source[:, lanes], share[:, lanes], jnp.zeros((6, 128), f32)], axis=0
            )
        tables[z] = table[z]

        for r in range(1, NZ):
            send(table_copy(r))

    def main():
        nbuf[0, 0] = normed_ref[:, :half]
        nbuf[0, 1] = normed_ref[:, half:]
        for hf in (0, 1):
            send(pass_on(0, up, hf, 1))
            send(pass_on(0, down, hf, -1))

        for copy in loads[:3]:
            copy.wait()
        n = normed_ref[...]
        g = jnp.dot(n, sg[...], preferred_element_type=f32)
        u = jnp.dot(n, su[...], preferred_element_type=f32)
        hidden = (g / (1.0 + jnp.exp(-g)) * u).astype(bf16)
        for i in range(4):
            cols = slice(i * width // 4, (i + 1) * width // 4)
            total[:, cols] = stream_ref[:, cols].astype(f32) + jnp.dot(
                hidden, sd[:, cols], preferred_element_type=f32
            )

        pairs = ((1, 5), (2, 6), (3, 7), (4, 0))
        offset = {0: 0, 1: -1, 2: -2, 3: -3, 4: -4, 5: 1, 6: 2, 7: 3}

        def arrive(slot, step, send_on, hf):
            if slot == UP_STEPS:
                pass_on(3 if hf == 0 else 7, slot, hf, 1 if hf == 0 else -1).wait_recv()
                return
            pass_on(slot - 1 if slot not in (up, down) else 0, slot, hf, step).wait_recv()
            if slot in (3, 7):
                if hf == (0 if slot == 3 else 1):
                    send(pass_on(slot, UP_STEPS, hf, step))
            elif send_on:
                send(pass_on(slot, slot + 1, hf, step))

        def x_copy(b, hf, r):
            to = (me8 + r) % 8
            return remote(
                sbuf.at[b, hf, to], xbuf.at[b, hf, me8], x_send.at[b, hf, r], x_recv.at[b, hf, r], zbase + to
            )

        def r_copy(b, hf, r):
            to = (me8 + r) % 8
            return remote(
                obuf.at[b, hf, to], rbuf.at[b, hf, me8], r_send.at[b, hf, r], r_recv.at[b, hf, r], zbase + to
            )

        def x_own(b, hf):
            return pltpu.make_async_copy(sbuf.at[b, hf, me8], xbuf.at[b, hf, me8], x_sem.at[b, hf])

        def r_own(b, hf):
            return pltpu.make_async_copy(obuf.at[b, hf, me8], rbuf.at[b, hf, me8], r_sem.at[b, hf])

        def choose(b):
            first, second = pairs[b]
            ta = tables[(z + offset[first] + NZ) % NZ]
            tb = tables[(z + offset[second] + NZ) % NZ]
            lane_of = lax.broadcasted_iota(jnp.int32, (1, 128), 1) % 16
            src = jnp.where(lane_of < 8, ta[0:1], tb[0:1] + 64.0)
            share_row = jnp.where(lane_of < 8, ta[1:2], tb[1:2])
            token_of = lax.broadcasted_iota(jnp.int32, (128, 128), 0).astype(f32)
            chosen = jnp.where(token_of == src, 1.0, 0.0)
            sel[...] = chosen.T.astype(bf16)
            gate[b] = (chosen * share_row).astype(bf16)

        def dispatch(b, hf):
            first, second = pairs[b]
            for i in range(2):
                cols = slice(i * half // 2, (i + 1) * half // 2)
                tokens = jnp.concatenate([nbuf[first, hf, :, cols], nbuf[second, hf, :, cols]], axis=0)
                picked = jnp.dot(sel[...], tokens, preferred_element_type=f32)
                sbuf[b, hf, :, :, cols] = picked.astype(bf16).reshape(8, 16, half // 2)
            for r in (4, 3, 5, 2, 6, 1, 7):
                send(x_copy(b, hf, r))
            x_own(b, hf).start()

        def give_back(b, hf):
            for r in (4, 3, 5, 2, 6, 1, 7):
                send(r_copy(b, hf, r))
            r_own(b, hf).start()

        def run_expert(b, give):
            g = u = None
            for hf in (0, 1):
                for r in range(1, 8):
                    x_copy(b, hf, r).wait_recv()
                x_own(b, hf).wait()
                rows_in = xbuf[b, hf].reshape(128, half)
                deep = slice(hf * half, (hf + 1) * half)
                g_part = jnp.dot(rows_in, eg[deep, :], preferred_element_type=f32)
                u_part = jnp.dot(rows_in, eu[deep, :], preferred_element_type=f32)
                g = g_part if g is None else g + g_part
                u = u_part if u is None else u + u_part
            hidden = (g / (1.0 + jnp.exp(-g)) * u).astype(bf16)
            for hf in (0, 1):
                for i in range(2):
                    cols = slice(i * half // 2, (i + 1) * half // 2)
                    at = hf * half + i * half // 2
                    made = jnp.dot(hidden, ed[:, at : at + half // 2], preferred_element_type=f32)
                    obuf[b, hf, :, :, cols] = made.astype(bf16).reshape(8, 16, half // 2)
                if give:
                    give_back(b, hf)

        def need_tables(*steps):
            for r in steps:
                table_copy(r).wait_recv()

        for b, moves, steps in (
            (0, ((1, 1, True), (5, -1, True)), (1, 7)),
            (1, ((2, 1, True), (6, -1, True)), (2, 6)),
            (2, ((3, 1, True), (7, -1, True)), (3, 5)),
            (3, ((4, 1, False),), (4,)),
        ):
            for hf in (0, 1):
                for slot, step, send_on in moves:
                    arrive(slot, step, send_on, hf)
                if hf == 0:
                    need_tables(*steps)
                    choose(b)
                dispatch(b, hf)
            if b == 0:
                for copy in loads[3:]:
                    copy.wait()
            else:
                run_expert(b - 1, False)
        run_expert(3, True)
        for b in (2, 1, 0):
            for hf in (0, 1):
                give_back(b, hf)

        def chain_copy(way, place, hf):
            return remote(
                cout.at[way, place, hf],
                cin.at[way, place, hf],
                c_send.at[way, place, hf],
                c_recv.at[way, place, hf],
                at_z(-1 if way == 0 else 1),
            )

        for b, places in ((3, (3, None)), (2, (2, 2)), (1, (1, 1)), (0, (0, 0))):
            for hf in (0, 1):
                for r in range(1, 8):
                    r_copy(b, hf, r).wait_recv()
                r_own(b, hf).wait()
                cols = slice(hf * half, (hf + 1) * half)
                part = jnp.dot(
                    gate[b], rbuf[b, hf].reshape(128, half), preferred_element_type=f32
                )
                for way in (0, 1):
                    mine = part[way * 64 : (way + 1) * 64]
                    place = places[way]
                    if place is None:
                        total[:, cols] = total[:, cols] + mine
                        continue
                    side = way if place < 3 else hf
                    if place < 2 or (place == 2 and hf == way):
                        chain_copy(side, place + 1, hf).wait_recv()
                        mine = mine + cin[side, place + 1, hf].astype(f32)
                    cout[side, place, hf] = mine.astype(bf16)
                    send(chain_copy(side, place, hf))
        for hf in (0, 1):
            cols = slice(hf * half, (hf + 1) * half)
            for way in (0, 1):
                chain_copy(way, 0, hf).wait_recv()
            out_ref[:, cols] = (
                total[:, cols] + cin[0, 0, hf].astype(f32) + cin[1, 0, hf].astype(f32)
            ).astype(bf16)
        for copy in sent:
            copy.wait_send()

    return prepare, main


def layer_kernel(*refs):
    att_in, (ids, route), weights = refs[:7], refs[7:9], refs[9:15]
    out, stream, normed = refs[15:18]
    att_scratch, scratch = refs[18 : 18 + ATTENTION_SCRATCH], refs[18 + ATTENTION_SCRATCH :]
    prepare, main = experts_parts(normed, stream, ids, route, *weights, out, *scratch)
    attention_kernel(prepare, *att_in, stream, normed, *att_scratch)
    main()


ATTENTION_SCRATCH = 38


def layer(
    residual,
    queries,
    key_rows,
    value_rows,
    forget_sums,
    out_weight,
    norm_gain,
    expert_ids,
    route_weights,
    expert_gate,
    expert_up,
    expert_down,
    shared_gate,
    shared_up,
    shared_down,
):
    rows, width = residual.shape
    tokens = queries.shape[0]
    hidden = expert_gate.shape[2]
    shared = shared_gate.shape[1]
    bf16, f32 = jnp.bfloat16, jnp.float32
    anywhere = pl.BlockSpec(memory_space=pl.ANY)
    vmem = pl.BlockSpec(memory_space=pltpu.VMEM)
    dma = pltpu.SemaphoreType.DMA
    return pl.pallas_call(
        layer_kernel,
        out_shape=jax.ShapeDtypeStruct((rows, width), bf16),
        in_specs=[vmem] * 4 + [anywhere] * 3 + [vmem] * 2 + [anywhere] * 6,
        out_specs=vmem,
        scratch_shapes=[
            pltpu.VMEM((rows, width), bf16),
            pltpu.VMEM((rows, width), bf16),
            pltpu.VMEM((2, 256, tokens), bf16),
            pltpu.VMEM((2, 128, tokens), bf16),
            pltpu.VMEM((8, 256, 256), bf16),
            pltpu.VMEM((8, 8, 256), f32),
            pltpu.VMEM((8, 2, 256, 128), bf16),
            pltpu.VMEM((8, 2, 128, 256), bf16),
            pltpu.VMEM((8, 2, 8, 256), f32),
            pltpu.VMEM((2, 8, 256), f32),
            pltpu.VMEM((8, 2, 256, 128), bf16),
            pltpu.VMEM((2, 128, 256), bf16),
            pltpu.VMEM((2, 2, 256, 256), f32),
            pltpu.VMEM((2, 2, 256, 256), f32),
            pltpu.VMEM((64, 2048), bf16),
            pltpu.VMEM((1, 2048), f32),
            pltpu.VMEM((8, 2, 128, 256), f32),
            pltpu.VMEM((8, 8, 256), f32),
            pltpu.VMEM((8, 256, 256), bf16),
            pltpu.VMEM((8, 2, 8, 128), f32),
            pltpu.VMEM((4, 8, 64, 256), bf16),
            pltpu.VMEM((4, 8, 8, 128), f32),
            pltpu.VMEM((4, 128, 128), f32),
            pltpu.VMEM((64, 2048), bf16),
            pltpu.VMEM((4, 512, 2048), bf16),
            dma((2, 8)),
            dma((2, 8)),
            dma((3, 8, 2)),
            dma((3, 8, 2)),
            dma((8, 4)),
            dma((8, 4)),
            dma((8, 4)),
            dma((8, 4)),
            dma((9,)),
            dma((9,)),
            dma((3, NY)),
            dma((3, NY)),
            dma((3, 2)),
            dma((3, 2)),
            dma((10,)),
            pltpu.VMEM((8, 2, rows, width // 2), bf16),
            pltpu.VMEM((8, 8, 128), f32),
            pltpu.VMEM((8, 8, 128), f32),
            pltpu.VMEM((128, 128), bf16),
            pltpu.VMEM((4, 128, 128), bf16),
            pltpu.VMEM((4, 2, 8, 16, width // 2), bf16),
            pltpu.VMEM((4, 2, 8, 16, width // 2), bf16),
            pltpu.VMEM((4, 2, 8, 16, width // 2), bf16),
            pltpu.VMEM((4, 2, 8, 16, width // 2), bf16),
            pltpu.VMEM((2, 4, 2, rows, width // 2), bf16),
            pltpu.VMEM((2, 4, 2, rows, width // 2), bf16),
            pltpu.VMEM((rows, width), f32),
            pltpu.VMEM((width, hidden), bf16),
            pltpu.VMEM((width, hidden), bf16),
            pltpu.VMEM((hidden, width), bf16),
            pltpu.VMEM((width, shared), bf16),
            pltpu.VMEM((width, shared), bf16),
            pltpu.VMEM((shared, width), bf16),
            dma((8, 2)),
            dma((8, 2)),
            dma((8,)),
            dma((8,)),
            dma((4, 2, 8)),
            dma((4, 2, 8)),
            dma((4, 2, 8)),
            dma((4, 2, 8)),
            dma((2, 4, 2)),
            dma((2, 4, 2)),
            dma((6,)),
            dma((4, 2)),
            dma((4, 2)),
        ],
        compiler_params=pltpu.CompilerParams(
            collective_id=0, has_side_effects=True, vmem_limit_bytes=66_000_000
        ),
        cost_estimate=pl.CostEstimate(
            flops=12 * 10**9, bytes_accessed=32 * 2**20, transcendentals=16 * 2**20
        ),
    )(
        queries,
        key_rows,
        value_rows,
        forget_sums.T,
        out_weight,
        residual,
        norm_gain.reshape(1, width),
        expert_ids.T,
        route_weights.T,
        expert_gate,
        expert_up,
        expert_down,
        shared_gate,
        shared_up,
        shared_down,
    )


def solution(mesh):
    in_specs = (
        P(("sp", "tp"), None),
        P("sp", "tp"),
        P("sp", "tp"),
        P("sp", "tp"),
        P("sp", "tp"),
        P("tp", None),
        P(),
        P(("sp", "tp"), None),
        P(("sp", "tp"), None),
        P("sp", None, None),
        P("sp", None, None),
        P("sp", None, None),
        P(),
        P(),
        P(),
    )
    out_specs = P(("sp", "tp"), None)
    return jax.shard_map(layer, mesh=mesh, in_specs=in_specs, out_specs=out_specs, check_vma=False)
```
